768 devices in a mesh: sp: 48 (over z, x), tp: 16 (over y, core).
Axes of the slice: x: 4, y: 8, z: 12, core: 2. Of those that a mesh axis runs over, the one named last changes fastest.
Arguments:
- tokens: bfloat16 [48, 480, 4096], P(None, 'sp', 'tp'), may hold values from -6 to 6
- latent_down_weight: bfloat16 [4096, 512], replicated, may hold values from -0.09375 to 0.09375
- w_rope_key: bfloat16 [4096, 64], replicated, may hold values from -0.09375 to 0.09375
- latent_norm_gain: float32 [512], replicated, may hold values from 0.1 to 1.9
- key_up_weight: bfloat16 [512, 4096], P(None, 'tp'), may hold values from -0.25 to 0.25
- value_up_weight: bfloat16 [512, 4096], P(None, 'tp'), may hold values from -0.25 to 0.25
- cached_latent_rows: bfloat16 [48, 32768, 512], P('sp', 'tp'), may hold values from -6 to 6
- past_rope: bfloat16 [48, 32768, 64], P('sp', 'tp'), may hold values from -6 to 6
- query_nope: bfloat16 [48, 4096], P('sp', 'tp'), may hold values from -8 to 8
- query_rope: bfloat16 [48, 2048], P('sp', 'tp'), may hold values from -300 to 300
Outputs:
- new_keys: bfloat16 [48, 480, 4096], P('sp', None, 'tp')
- new_values: bfloat16 [48, 480, 4096], P('sp', None, 'tp')
- new_rope: bfloat16 [48, 480, 64], P('sp')
- attended: bfloat16 [48, 4096], P('sp', 'tp')
The draws below stay inside these ranges and needn't reach their ends.
All inputs are finite; a program needn't handle non-finite values.
Results may differ from the reference program's by a relative error of at most 0.0085.
Values may be sent and summed in bfloat16 or wider, within the bound.
No kernel may reach another device: no remote copies, remote signals or barrier semaphores. Data moves between devices by JAX's collectives and lax.ppermute only.
A program may use at most 64 MiB of HBM per device.

```python
import jax
import jax.numpy as jnp
from jax import lax

MODEL_WIDTH = 4096
HEAD_COUNT = 32
LATENT_WIDTH = 512
PLAIN_KEY_WIDTH = 128
ROPE = 64
VALUE_WIDTH = 128
PAST_POSITIONS = 32768
PROMPT_COUNT = 48
NEW = 480


def drawn_turn(key):
    turn = jnp.clip(jax.random.normal(jax.random.fold_in(key, 21), (PROMPT_COUNT, PAST_POSITIONS, ROPE), jnp.float32), -6.0, 6.0)
    return turn


def draw_past_rope(key, part):
    return drawn_turn(key).astype(jnp.bfloat16)


def draw_query_rope(key, part):
    return jnp.clip(1.5 * jax.random.normal(jax.random.fold_in(key, 25), (PROMPT_COUNT, HEAD_COUNT * ROPE), jnp.float32), -9.0, 9.0).astype(jnp.bfloat16)


def steps_of(rng, shape, shards, least, largest):
    factor_of = 1.0
    for axis_at, parts in shards:
        draws = jax.random.uniform(jax.random.fold_in(jax.random.fold_in(rng, 6), axis_at), (parts,), jnp.float32, least / len(shards), largest / len(shards))
        factor_of = factor_of * jnp.repeat(jnp.exp(draws), shape[axis_at] // parts).reshape((-1,) + (1,) * (len(shape) - 1 - axis_at))
    return factor_of


def gaussian(stream_key, extent, deviation, bound, shards=(), kind=jnp.bfloat16):
    result = deviation * jax.random.normal(stream_key, extent, jnp.float32)
    if shards:
        result = result * steps_of(stream_key, extent, shards, -0.22, 0.18)
    return jnp.clip(result, -bound, bound).astype(kind)


def setup_inputs(seed: int = 0) -> dict:
    seeds = jax.random.split(jax.random.key(seed), 11)
    tokens = gaussian(seeds[0], (PROMPT_COUNT, NEW, MODEL_WIDTH), 1.0, 6.0, ((1, 48), (2, 16)))
    latent_down_weight = gaussian(seeds[1], (MODEL_WIDTH, LATENT_WIDTH), MODEL_WIDTH ** -0.5, 0.09375)
    w_rope_key = gaussian(seeds[2], (MODEL_WIDTH, ROPE), MODEL_WIDTH ** -0.5, 0.09375)
    latent_norm_gain = jnp.clip(1.0 + 0.18 * jax.random.normal(seeds[3], (LATENT_WIDTH,), jnp.float32), 0.1, 1.9)
    key_up_weight = gaussian(seeds[4], (LATENT_WIDTH, HEAD_COUNT * PLAIN_KEY_WIDTH), LATENT_WIDTH ** -0.5, 0.25, ((1, 16),))
    value_up_weight = gaussian(seeds[5], (LATENT_WIDTH, HEAD_COUNT * VALUE_WIDTH), LATENT_WIDTH ** -0.5, 0.25, ((1, 16),))
    cached_latent_rows = gaussian(seeds[6], (PROMPT_COUNT, PAST_POSITIONS, LATENT_WIDTH), 1.0, 6.0, ((0, 48), (1, 16)))
    past_rope = draw_past_rope(jax.random.fold_in(seeds[10], 71), 0)
    query_nope = gaussian(seeds[8], (PROMPT_COUNT, HEAD_COUNT * PLAIN_KEY_WIDTH), 1.5, 8.0, ((0, 48), (1, 16)))
    query_rope = draw_query_rope(jax.random.fold_in(seeds[10], 71), 0)
    return dict(tokens=tokens, latent_down_weight=latent_down_weight, w_rope_key=w_rope_key, latent_norm_gain=latent_norm_gain, key_up_weight=key_up_weight, value_up_weight=value_up_weight, cached_latent_rows=cached_latent_rows, past_rope=past_rope, query_nope=query_nope, query_rope=query_rope)


epsilon = 1e-06
rope_theta = 10000.0

def rotate(values, positions):
    halfway = values.shape[-1] // 2
    frequency = rope_theta ** (-jnp.arange(halfway, dtype=jnp.float32) / halfway)
    angles = positions[:, None] * frequency
    first = values[..., :halfway]
    second = values[..., halfway:]
    return jnp.concatenate([first * jnp.cos(angles) - second * jnp.sin(angles), first * jnp.sin(angles) + second * jnp.cos(angles)], axis=-1)

def reference(tokens, latent_down_weight, w_rope_key, latent_norm_gain, key_up_weight, value_up_weight, cached_latent_rows, past_rope, query_nope, query_rope):
    flat = tokens.reshape(PROMPT_COUNT * NEW, MODEL_WIDTH)
    latent_raw = jnp.dot(flat, latent_down_weight, preferred_element_type=jnp.float32)
    rope_raw = jnp.dot(flat, w_rope_key, preferred_element_type=jnp.float32)
    scale = lax.rsqrt(lax.optimization_barrier(jnp.mean(latent_raw * latent_raw, axis=-1, keepdims=True)) + epsilon)
    latent = (latent_raw * scale * latent_norm_gain.astype(jnp.float32)).astype(jnp.bfloat16)
    positions = (PAST_POSITIONS + jnp.arange(NEW)).astype(jnp.float32)
    new_rope = rotate(rope_raw.reshape(PROMPT_COUNT, NEW, ROPE), positions).astype(jnp.bfloat16)
    new_keys = jnp.dot(latent, key_up_weight, preferred_element_type=jnp.float32).astype(jnp.bfloat16).reshape(PROMPT_COUNT, NEW, HEAD_COUNT * PLAIN_KEY_WIDTH)
    new_values = jnp.dot(latent, value_up_weight, preferred_element_type=jnp.float32).astype(jnp.bfloat16).reshape(PROMPT_COUNT, NEW, HEAD_COUNT * VALUE_WIDTH)
    head_keys = key_up_weight.reshape(LATENT_WIDTH, HEAD_COUNT, PLAIN_KEY_WIDTH).astype(jnp.float32)
    head_values = value_up_weight.reshape(LATENT_WIDTH, HEAD_COUNT, VALUE_WIDTH).astype(jnp.float32)
    factor = (PLAIN_KEY_WIDTH + ROPE) ** (-0.5)

    def read_sequence(items):
        query_heads, query_turn, cached, cached_turn, fresh_keys, fresh_values, fresh_turn = items
        query_heads = query_heads.astype(jnp.float32)
        query_turn = query_turn.astype(jnp.float32)
        query_latent = jnp.einsum('hd,khd->hk', query_heads, head_keys).astype(jnp.bfloat16).astype(jnp.float32)
        cached = cached.astype(jnp.float32)
        past_scores = (jnp.einsum('hk,pk->hp', query_latent, cached) + jnp.einsum('hd,pd->hp', query_turn, cached_turn.astype(jnp.float32))) * factor
        new_scores = (jnp.einsum('hd,phd->hp', query_heads, fresh_keys.astype(jnp.float32)) + jnp.einsum('hd,pd->hp', query_turn, fresh_turn.astype(jnp.float32))) * factor
        peak = jnp.maximum(lax.optimization_barrier(jnp.max(past_scores, axis=-1)), lax.optimization_barrier(jnp.max(new_scores, axis=-1)))
        past_weight = jnp.exp(past_scores - peak[:, None])
        new_weight = jnp.exp(new_scores - peak[:, None])
        denominator = lax.optimization_barrier(jnp.sum(past_weight, axis=-1)) + lax.optimization_barrier(jnp.sum(new_weight, axis=-1))
        latent_sum = jnp.einsum('hp,pk->hk', past_weight.astype(jnp.bfloat16).astype(jnp.float32), cached)
        latent_sum = latent_sum.astype(jnp.bfloat16).astype(jnp.float32)
        past_out = jnp.einsum('hk,khd->hd', latent_sum, head_values)
        new_out = jnp.einsum('hp,phd->hd', new_weight.astype(jnp.bfloat16).astype(jnp.float32), fresh_values.astype(jnp.float32))
        return ((past_out + new_out) / denominator[:, None]).astype(jnp.bfloat16).reshape(HEAD_COUNT * VALUE_WIDTH)
    attended = lax.map(read_sequence, (query_nope.reshape(PROMPT_COUNT, HEAD_COUNT, PLAIN_KEY_WIDTH), query_rope.reshape(PROMPT_COUNT, HEAD_COUNT, ROPE), cached_latent_rows, past_rope, new_keys.reshape(PROMPT_COUNT, NEW, HEAD_COUNT, PLAIN_KEY_WIDTH), new_values.reshape(PROMPT_COUNT, NEW, HEAD_COUNT, VALUE_WIDTH), new_rope))
    return (new_keys, new_values, new_rope, attended)
```

```python
import jax
import jax.numpy as jnp
from jax import lax
from jax.sharding import Mesh
from jax.sharding import PartitionSpec as P

PLAIN_KEY_WIDTH = 128
ROPE = 64
VALUE_WIDTH = 128
PAST_POSITIONS = 32768
TP = ("tp_0", "tp_1")
BLOCK = 32


epsilon = 1e-06
rope_theta = 10000.0


def rotate(values, positions):
    halfway = values.shape[-1] // 2
    frequency = rope_theta ** (-jnp.arange(halfway, dtype=jnp.float32) / halfway)
    angles = positions[:, None] * frequency
    first = values[..., :halfway]
    second = values[..., halfway:]
    return jnp.concatenate(
        [
            first * jnp.cos(angles) - second * jnp.sin(angles),
            first * jnp.sin(angles) + second * jnp.cos(angles),
        ],
        axis=-1,
    )


def split_parts(x, count):
    parts = []
    for _ in range(count - 1):
        part = lax.reduce_precision(x, 8, 7)
        parts.append(part.astype(jnp.bfloat16))
        x = x - part
    parts.append(x.astype(jnp.bfloat16))
    return parts


def on_device(
    tokens,
    latent_down_weight,
    w_rope_key,
    latent_norm_gain,
    key_up_weight,
    value_up_weight,
    cached_latent_rows,
    past_rope,
    query_nope,
    query_rope,
):
    f32, bf16 = jnp.float32, jnp.bfloat16
    factor = (PLAIN_KEY_WIDTH + ROPE) ** (-0.5)
    latent_width = latent_down_weight.shape[1]
    features = tokens.shape[2]
    heads = query_nope.shape[1] // PLAIN_KEY_WIDTH
    ranks = lax.axis_size(TP)
    pairs = lax.axis_size("tp_1")
    rings = ranks // pairs
    rank = lax.axis_index(TP)

    arrived = lax.all_to_all(tokens, "sp", split_axis=0, concat_axis=0, tiled=True)
    rows = arrived.reshape(-1, features)
    row_count = rows.shape[0]

    query_own = query_nope.reshape(heads, PLAIN_KEY_WIDTH)
    turn_own = query_rope.reshape(heads, ROPE)
    head_keys = key_up_weight.reshape(latent_width, heads, PLAIN_KEY_WIDTH)
    query_latent = jnp.einsum(
        "hd,khd->hk", query_own, head_keys, preferred_element_type=f32
    ).astype(bf16)

    latent_lines = heads * latent_width // features
    extra = 8
    query_lines = jnp.concatenate(
        [
            query_latent.reshape(latent_lines, features),
            jnp.pad(turn_own.reshape(1, -1), ((0, 0), (0, features - heads * ROPE))),
            jnp.zeros((extra - latent_lines - 1, features), bf16),
        ]
    )
    block = BLOCK
    workers = row_count // block
    blocks = jnp.pad(rows.reshape(workers, block, features), ((0, ranks - workers), (0, 0), (0, 0)))
    outgoing = jnp.concatenate(
        [blocks, jnp.broadcast_to(query_lines, (ranks, extra, features))], axis=1
    )
    whole = lax.all_to_all(outgoing, TP, split_axis=0, concat_axis=0, tiled=True)
    x = whole[:, :block].transpose(1, 0, 2).reshape(block, ranks * features)
    latent_raw = jnp.dot(x, latent_down_weight, preferred_element_type=f32)
    rope_raw = jnp.dot(x, w_rope_key, preferred_element_type=f32)
    scale = lax.rsqrt(jnp.mean(latent_raw * latent_raw, axis=-1, keepdims=True) + epsilon)
    latent_own = (latent_raw * scale * latent_norm_gain).astype(bf16)
    positions = (PAST_POSITIONS + rank * block + jnp.arange(block)).astype(f32)
    rope_own = rotate(rope_raw, positions).astype(bf16)

    every_latent = whole[:, block : block + latent_lines].reshape(ranks * heads, latent_width)
    every_turn = whole[:, block + latent_lines, : heads * ROPE].reshape(ranks * heads, ROPE)
    cached = cached_latent_rows[0]
    past_scores = jnp.einsum("hk,pk->hp", every_latent, cached, preferred_element_type=f32)
    past_scores = (
        past_scores + jnp.einsum("hd,pd->hp", every_turn, past_rope[0], preferred_element_type=f32)
    ) * factor
    local_peak = jnp.max(past_scores, axis=-1)
    local_weight = jnp.exp(past_scores - local_peak[:, None])
    local_total = jnp.sum(local_weight, axis=-1)
    local_latent = jnp.einsum(
        "hp,pk->hk", local_weight.astype(bf16), cached, preferred_element_type=f32
    )

    group = pairs * heads
    stats = jnp.stack(split_parts(local_peak, 3) + split_parts(local_total, 3))
    stats = stats.reshape(6, rings, group).transpose(1, 0, 2).reshape(rings, 1, 6 * group)
    stats = jnp.pad(stats, ((0, 0), (0, 0), (0, latent_width - 6 * group)))
    sums = [p.reshape(rings, group, latent_width) for p in split_parts(local_latent, 2)]
    turn_lines = block * ROPE // latent_width
    fixed = jnp.concatenate([latent_own, rope_own.reshape(turn_lines, latent_width)])
    chunk = jnp.concatenate(
        [jnp.broadcast_to(fixed, (rings, *fixed.shape)), *sums, stats], axis=1
    )
    chunk = jnp.pad(chunk, ((0, 0), (0, -chunk.shape[1] % 8), (0, 0)))
    got = lax.all_to_all(chunk, "tp_0", split_axis=0, concat_axis=0, tiled=True)
    both = lax.all_gather(got, "tp_1")

    ordered = both[:, :, : block + turn_lines].transpose(1, 0, 2, 3)
    ordered = ordered.reshape(ranks, block + turn_lines, latent_width)[:workers]
    latent = ordered[:, :block].reshape(row_count, latent_width)
    new_rope = ordered[:, block:].reshape(row_count, ROPE)
    at = block + turn_lines
    own = lax.axis_index("tp_1") * heads
    high = lax.dynamic_slice_in_dim(both[:, :, at : at + group], own, heads, 2)
    low = lax.dynamic_slice_in_dim(both[:, :, at + group : at + 2 * group], own, heads, 2)
    sums_all = high.astype(f32) + low.astype(f32)
    numbers = both[:, :, at + 2 * group, : 6 * group].reshape(pairs, rings, 6, group).astype(f32)
    numbers = lax.dynamic_slice_in_dim(numbers, own, heads, 3)
    peaks = numbers[:, :, 0] + numbers[:, :, 1] + numbers[:, :, 2]
    totals = numbers[:, :, 3] + numbers[:, :, 4] + numbers[:, :, 5]

    new_keys = jnp.dot(latent, key_up_weight, preferred_element_type=f32).astype(bf16)
    new_values = jnp.dot(latent, value_up_weight, preferred_element_type=f32).astype(bf16)

    new_scores = jnp.einsum(
        "hd,phd->hp",
        query_own,
        new_keys.reshape(row_count, heads, PLAIN_KEY_WIDTH),
        preferred_element_type=f32,
    )
    new_scores = (
        new_scores + jnp.einsum("hd,pd->hp", turn_own, new_rope, preferred_element_type=f32)
    ) * factor
    peak = jnp.maximum(jnp.max(peaks, axis=(0, 1)), jnp.max(new_scores, axis=-1))
    share = jnp.exp(peaks - peak)
    new_weight = jnp.exp(new_scores - peak[:, None])
    denominator = jnp.sum(totals * share, axis=(0, 1)) + jnp.sum(new_weight, axis=-1)
    latent_sum = jnp.sum(sums_all * share[..., None], axis=(0, 1)).astype(bf16)
    head_values = value_up_weight.reshape(latent_width, heads, VALUE_WIDTH)
    past_out = jnp.einsum("hk,khd->hd", latent_sum, head_values, preferred_element_type=f32)
    new_out = jnp.einsum(
        "hp,phd->hd",
        new_weight.astype(bf16),
        new_values.reshape(row_count, heads, VALUE_WIDTH),
        preferred_element_type=f32,
    )
    attended = ((past_out + new_out) / denominator[:, None]).astype(bf16).reshape(1, -1)
    return (new_keys[None], new_values[None], new_rope[None], attended)


def solution(mesh):
    split = Mesh(mesh.devices.reshape(mesh.shape["sp"], 8, 2), ("sp", "tp_0", "tp_1"))
    return jax.shard_map(
        on_device,
        mesh=split,
        in_specs=(
            P(None, "sp", TP),
            P(),
            P(),
            P(),
            P(None, TP),
            P(None, TP),
            P("sp", TP, None),
            P("sp", TP, None),
            P("sp", TP),
            P("sp", TP),
        ),
        out_specs=(P("sp", None, TP), P("sp", None, TP), P("sp", None, None), P("sp", TP)),
        check_vma=False,
    )
```

```python
import jax
import jax.numpy as jnp
import numpy as np
from jax import lax
from jax.experimental import pallas as pl
from jax.experimental.pallas import tpu as pltpu
from jax.sharding import Mesh
from jax.sharding import PartitionSpec as P

PLAIN_KEY_WIDTH = 128
ROPE = 64
VALUE_WIDTH = 128
PAST_POSITIONS = 32768
TP = ("tp_0", "tp_1")
EXTRA = 16
TILE = 8
FACTOR = (PLAIN_KEY_WIDTH + ROPE) ** (-0.5)

epsilon = 1e-06
rope_theta = 10000.0

VMEM = pl.BlockSpec(memory_space=pltpu.VMEM)
HBM = pl.BlockSpec(memory_space=pltpu.HBM)
MIB = 1 << 20
f32, bf16 = jnp.float32, jnp.bfloat16
NT = (((1,), (1,)), ((), ()))


def mm(a, b):
    return jnp.dot(a, b, preferred_element_type=f32)


def mm_nt(a, b):
    return lax.dot_general(a, b, NT, preferred_element_type=f32)


def iota(shape, dim):
    return lax.broadcasted_iota(jnp.int32, shape, dim)


def by_head(row, width):
    shape = (TILE, row.shape[1])
    spread = jnp.broadcast_to(row.astype(f32), shape)
    return jnp.where(iota(shape, 1) // width == iota(shape, 0), spread, 0.0).astype(bf16)


def three(x):
    high = x.astype(bf16).astype(f32)
    rest = x - high
    middle = rest.astype(bf16).astype(f32)
    return high, middle, rest - middle


def pack_kernel(
    tokens_hbm,
    nope_hbm,
    turn_hbm,
    key_hbm,
    angle_ref,
    out_ref,
    angle_out_ref,
    nope_ref,
    turn_ref,
    key_ref,
    sem,
):
    needed = [
        pltpu.make_async_copy(source, target, sem.at[k])
        for k, (source, target) in enumerate(
            ((key_hbm, key_ref), (nope_hbm, nope_ref), (turn_hbm, turn_ref))
        )
    ]
    for copy in needed:
        copy.start()
    angle_out_ref[...] = angle_ref[...]
    rings, lines, half = out_ref.shape
    prompts = tokens_hbm.shape[1]
    copies = [pltpu.make_async_copy(tokens_hbm.at[:rings], out_ref.at[:, :prompts], sem.at[3])]
    last = prompts // EXTRA - 1
    for y in range(rings):
        third = jnp.minimum(lax.rem(y % (rings // 2) + lax.axis_index("sp"), rings // 2), last)
        part = pl.ds(pl.multiple_of(third * EXTRA, EXTRA), EXTRA)
        source = tokens_hbm.at[rings + y // (rings // 2), part]
        target = out_ref.at[y, prompts : prompts + EXTRA]
        copies.append(pltpu.make_async_copy(source, target, sem.at[4 + y]))
    for copy in copies:
        copy.start()
    for copy in needed:
        copy.wait()
    latent = mm_nt(by_head(nope_ref[...], PLAIN_KEY_WIDTH), key_ref[...])
    turn = turn_ref[...].astype(f32)
    blank = jnp.zeros((1, half - ROPE), f32)
    query = [latent[0:2, :half], latent[0:2, half:]]
    query += [jnp.concatenate([turn[:, h * ROPE : (h + 1) * ROPE], blank], axis=1) for h in (0, 1)]
    query.append(jnp.zeros((2, half), f32))
    query = jnp.concatenate(query, axis=0).astype(bf16)
    for y in range(rings):
        out_ref[y, lines - TILE :, :] = query
    for copy in copies:
        copy.wait()


def project_kernel(
    rows_ref,
    angle_ref,
    turn_down_hbm,
    gain_hbm,
    down_hbm,
    out_ref,
    line_ref,
    turn_down_ref,
    gain_ref,
    down_ref,
    sem,
):
    ranks, _, features = rows_ref.shape
    rings = ranks // 2
    prompts, tiles, lanes = out_ref.shape
    count = prompts + EXTRA
    width = down_ref.shape[1]
    copies = [
        pltpu.make_async_copy(turn_down_hbm, turn_down_ref, sem.at[0]),
        pltpu.make_async_copy(gain_hbm, gain_ref, sem.at[1]),
    ]
    for y in range(rings):
        part = pl.ds(2 * y * features, 2 * features)
        copies.append(pltpu.make_async_copy(down_hbm.at[part], down_ref.at[part], sem.at[2 + y]))
    for copy in copies:
        copy.start()
    line_ref[...] = jnp.zeros_like(line_ref)
    raw = jnp.zeros((count, width), f32)
    turned = jnp.zeros((count, ROPE), f32)
    copies[0].wait()
    copies[1].wait()
    for t in range(ranks):
        x = rows_ref[(t % 2) * rings + t // 2, :count, :]
        turned = turned + mm_nt(x, turn_down_ref[:, t * features : (t + 1) * features])
    for t in range(ranks):
        if t % 2 == 0:
            copies[2 + t // 2].wait()
        x = rows_ref[(t % 2) * rings + t // 2, :count, :]
        raw = raw + mm(x, down_ref[t * features : (t + 1) * features, :])
    scale = lax.rsqrt(jnp.mean(raw * raw, axis=-1, keepdims=True) + epsilon)
    latent = raw * scale * gain_ref[...]
    first, second = turned[:, : ROPE // 2], turned[:, ROPE // 2 :]
    full = iota((count, ROPE // 2), 0) < prompts
    cos = jnp.where(full, angle_ref[0, 0:1, :], angle_ref[0, 1:2, :])
    sin = jnp.where(full, angle_ref[1, 0:1, :], angle_ref[1, 1:2, :])
    turned = jnp.where(
        lax.axis_index("tp_1") == 0, first * cos - second * sin, first * sin + second * cos
    )
    half = width // 2
    own = jnp.where(lax.axis_index("tp_1") == 0, latent[:, :half], latent[:, half:])

    def repeated(x):
        return jnp.concatenate([x[prompts:]] * (prompts // EXTRA))

    parts = [own[:prompts, :lanes], own[:prompts, lanes:]]
    parts += [repeated(own[:, :lanes]), repeated(own[:, lanes:])]
    blank = jnp.zeros((prompts, lanes - ROPE), f32)
    parts.append(jnp.concatenate([turned[:prompts], repeated(turned), blank], axis=1))
    for k, part in enumerate(parts):
        line_ref[pl.ds(k, prompts, stride=tiles), :] = part
    out_ref[...] = line_ref[...].astype(bf16).reshape(out_ref.shape)


def past_kernel(rows_ref, cached_ref, past_ref, sums_ref, stats_ref):
    ranks, count, features = rows_ref.shape
    rings = ranks // 2
    width = cached_ref.shape[1]
    heads = 2 * ranks
    group = heads // rings
    lines = rows_ref[:, count - TILE :, :].reshape(ranks * TILE, features)
    shape = (heads, ranks * TILE)
    head, line = iota(shape, 0), iota(shape, 1)
    source = ((head // 2) % 2) * rings + head // 4

    def pick(first):
        wanted = source * TILE + first + head % 2
        return mm(jnp.where(line == wanted, 1.0, 0.0).astype(bf16), lines).astype(bf16)

    query = jnp.concatenate([pick(0), pick(2)], axis=1)
    turn = pick(4)[:, :ROPE]
    cached = cached_ref[...]
    score = (mm_nt(query, cached) + mm(turn, past_ref[...])) * FACTOR
    peak = jnp.max(score, axis=-1, keepdims=True)
    weight = jnp.exp(score - peak)
    total = jnp.sum(weight, axis=-1, keepdims=True)
    summed = mm(weight.astype(bf16), cached)
    high = summed.astype(bf16).astype(f32)
    low = summed - high

    shape = (heads, width // 2)
    column = iota(shape, 1) // 8 - 6 * (iota(shape, 0) % group)
    spread = jnp.zeros(shape, f32)
    for k, part in enumerate((*three(peak), *three(total))):
        spread = jnp.where(column == k, part, spread)
    shape = (rings, heads)
    wanted = jnp.where(iota(shape, 0) == iota(shape, 1) // group, 1.0, 0.0)
    numbers = mm(wanted.astype(bf16), spread.astype(bf16))
    for y in range(rings):
        at = slice(group * y, group * (y + 1))
        sums_ref[y] = jnp.concatenate([high[at], low[at]]).astype(bf16)
    stats_ref[...] = numbers


def chunk_kernel(lines_ref, sums_ref, stats_ref, out_ref, flat_ref):
    prompts, tiles, lanes = lines_ref.shape
    rings, lines, width = out_ref.shape
    turns = rings // 2
    flat_ref[...] = lines_ref[...].reshape(prompts * tiles, lanes).astype(f32)
    first = lax.rem(lax.axis_index("sp") // EXTRA + rings - lax.axis_index("tp_0"), turns)

    def some(k):
        return flat_ref[pl.ds(first * tiles + k, prompts // turns, stride=turns * tiles), :]

    full = [flat_ref[pl.ds(k, prompts, stride=tiles), :] for k in (0, 1, 4)]
    spare = EXTRA - prompts // turns
    stacked = jnp.concatenate(
        [
            jnp.concatenate(full[:2], axis=1),
            jnp.concatenate([some(2), some(3)], axis=1),
            jnp.zeros((spare, width // 2), f32),
        ]
    )
    count = stacked.shape[0] // 2
    latent = jnp.concatenate([stacked[:count], stacked[count:]], axis=1).astype(bf16)
    half = ROPE // 2
    turned = jnp.concatenate(
        [full[2][:, :half], some(4)[:, half:ROPE], jnp.zeros((spare, half), f32)]
    )
    turned = jnp.concatenate(
        [turned[TILE * k : TILE * (k + 1)] for k in range(2 * count // TILE)], axis=1
    )
    for y in range(rings):
        out_ref[y, :count, :] = latent
        out_ref[y, count : count + TILE, :] = sums_ref[y]
        numbers = jnp.concatenate(
            [stats_ref[y : y + 1, :], jnp.zeros((TILE - 1, width // 2), f32)]
        )
        out_ref[y, count + TILE :, :] = jnp.concatenate([turned, numbers], axis=1).astype(bf16)


def finish_kernel(
    both_ref,
    key_ref,
    value_hbm,
    nope_ref,
    turn_ref,
    place_ref,
    keys_ref,
    values_ref,
    rope_ref,
    out_ref,
    latent_ref,
    turned_ref,
    value_ref,
    sem,
):
    load = pltpu.make_async_copy(value_hbm, value_ref, sem)
    load.start()
    sources, lines, width = both_ref.shape
    rings = sources // 2
    count = lines - 2 * TILE
    rows = keys_ref.shape[0]
    group = 4
    half = ROPE // 2
    for y in range(rings):
        halves = []
        for c in range(2):
            source = c * rings + y
            columns = slice(c * width // 2, (c + 1) * width // 2)
            for upper in range(2):
                at = slice((2 * y + upper) * count, (2 * y + upper + 1) * count)
                latent_ref[at, columns] = both_ref[
                    source, :count, upper * width // 2 : (upper + 1) * width // 2
                ]
            packed = both_ref[source, count + TILE :, :].astype(f32)
            halves.append(
                jnp.concatenate(
                    [packed[:, half * k : half * (k + 1)] for k in range(2 * count // TILE)]
                )
            )
        at = slice(2 * y * count, 2 * (y + 1) * count)
        turned_ref[at, :] = jnp.concatenate(halves, axis=1).astype(bf16)

    third = lax.axis_index("sp") // EXTRA
    place = place_ref[0:1, :]
    for k in range(1, place_ref.shape[0]):
        place = jnp.where(third == k, place_ref[k : k + 1, :], place)
    held = latent_ref.shape[0]
    move = jnp.where(iota((rows, held), 0) == place, 1.0, 0.0).astype(bf16)
    latent = mm(move, latent_ref[...]).astype(bf16)
    turned = mm(move, turned_ref[...]).astype(bf16)
    keys = mm(latent, key_ref[...]).astype(bf16)
    keys_ref[...] = keys
    load.wait()
    values = mm(latent, value_ref[...]).astype(bf16)
    values_ref[...] = values
    same = jnp.where(iota((ROPE, ROPE), 0) == iota((ROPE, ROPE), 1), 1.0, 0.0).astype(bf16)
    rope = mm_nt(same, turned).astype(bf16)
    rope_ref[...] = rope

    nope = by_head(nope_ref[...], PLAIN_KEY_WIDTH)
    turn = by_head(turn_ref[...], ROPE)
    score = (mm_nt(nope, keys) + mm(turn, jnp.concatenate([rope, rope], axis=0))) * FACTOR

    shape = (group, width // 2)
    place = iota(shape, 1) // 8 - 6 * iota(shape, 0)
    mine = [(iota(shape, 1) % 8 == 0) & (place >= k) & (place < k + 3) for k in (0, 3)]
    peaks, totals = [], []
    for source in range(sources):
        numbers = both_ref[source, count + TILE :, width // 2 :].astype(f32)[:1]
        for found, where in zip((peaks, totals), mine):
            found.append(jnp.sum(jnp.where(where, numbers, 0.0), axis=-1, keepdims=True))
    past_peak = peaks[0]
    for x in peaks[1:]:
        past_peak = jnp.maximum(past_peak, x)
    past_total = jnp.zeros((group, 1), f32)
    past_sum = jnp.zeros((TILE, width), f32)
    for k in range(sources):
        share = jnp.exp(peaks[k] - past_peak)
        past_total = past_total + totals[k] * share
        sums = both_ref[k, count : count + TILE, :].astype(f32)
        past_sum = past_sum + sums * jnp.concatenate([share, share])
    past_sum = past_sum[:group] + past_sum[group:]

    def own(x):
        half = group // 2
        mine = jnp.where(lax.axis_index("tp_1") == 0, x[:half], x[half:])
        return jnp.concatenate([mine, jnp.zeros((TILE - half, x.shape[1]), f32)])

    past_peak, past_total, past_sum = own(past_peak), own(past_total), own(past_sum)
    peak = jnp.maximum(past_peak, jnp.max(score, axis=-1, keepdims=True))
    share = jnp.exp(past_peak - peak)
    weight = jnp.exp(score - peak)
    denominator = past_total * share + jnp.sum(weight, axis=-1, keepdims=True)
    result = mm((past_sum * share).astype(bf16), value_ref[...]) + mm(weight.astype(bf16), values)
    result = result / denominator
    shape = result.shape
    result = jnp.where(iota(shape, 1) // VALUE_WIDTH == iota(shape, 0), result, 0.0)
    out_ref[...] = jnp.sum(result, axis=0, keepdims=True).astype(bf16)


def shaped(shape, dtype=bf16):
    return jax.ShapeDtypeStruct(shape, dtype)


def limit(mib):
    return pltpu.CompilerParams(vmem_limit_bytes=mib * MIB)


def pinned(x):
    return pltpu.with_memory_space_constraint(x, pltpu.HBM)


def on_device(
    tokens,
    latent_down_weight,
    w_rope_key,
    latent_norm_gain,
    key_up_weight,
    value_up_weight,
    cached_latent_rows,
    past_rope,
    query_nope,
    query_rope,
):
    prompts, per_device, features = tokens.shape
    width = latent_down_weight.shape[1]
    row_count = prompts * per_device
    rings = lax.axis_size("tp_0")
    ring = lax.axis_index("tp_0")
    device = lax.axis_index("sp")

    places = jnp.stack([ring, rings + ring // (rings // 2)])
    positions = (PAST_POSITIONS + device * per_device + places).astype(f32)
    halfway = ROPE // 2
    frequency = rope_theta ** (-jnp.arange(halfway, dtype=f32) / halfway)
    angles = positions[:, None] * frequency

    turns = jnp.stack([jnp.cos(angles), jnp.sin(angles)])
    sources = (query_nope, query_rope, key_up_weight)
    outgoing, turns = pl.pallas_call(
        pack_kernel,
        out_shape=(shaped((rings, prompts + EXTRA + TILE, features)), shaped(turns.shape, f32)),
        in_specs=[HBM] * 4 + [VMEM],
        out_specs=(VMEM, VMEM),
        scratch_shapes=[pltpu.VMEM(x.shape, bf16) for x in sources]
        + [pltpu.SemaphoreType.DMA((4 + rings,))],
        name="pack",
        compiler_params=limit(4),
    )(pinned(tokens.transpose(1, 0, 2)), *(pinned(x) for x in sources), turns)
    rows = lax.all_to_all(outgoing, "tp_0", split_axis=0, concat_axis=0, tiled=True)
    rows = lax.all_gather(rows, "tp_1", axis=0, tiled=True)

    lanes = 128
    sources = (w_rope_key.T, latent_norm_gain[None], latent_down_weight)
    lines = pl.pallas_call(
        project_kernel,
        out_shape=shaped((prompts, TILE, lanes)),
        in_specs=[VMEM] * 2 + [HBM] * 3,
        out_specs=VMEM,
        scratch_shapes=[pltpu.VMEM((prompts * TILE, lanes), f32)]
        + [pltpu.VMEM(x.shape, x.dtype) for x in sources]
        + [pltpu.SemaphoreType.DMA((rings + 2,))],
        name="project",
        compiler_params=limit(12),
    )(rows, turns, *(pinned(x) for x in sources))
    arrived = lax.all_to_all(lines, "sp", split_axis=0, concat_axis=0, tiled=True)

    sums, stats = pl.pallas_call(
        past_kernel,
        out_shape=(shaped((rings, TILE, width)), shaped((rings, width // 2), f32)),
        in_specs=[VMEM] * 3,
        out_specs=(VMEM, VMEM),
        name="past",
        compiler_params=limit(4),
        cost_estimate=pl.CostEstimate(
            flops=300_000_000, bytes_accessed=4 * MIB, transcendentals=65536
        ),
    )(rows, cached_latent_rows[0], past_rope[0].T)

    count = prompts + EXTRA
    chunk = pl.pallas_call(
        chunk_kernel,
        out_shape=shaped((rings, count // 2 + 2 * TILE, width)),
        in_specs=[VMEM] * 3,
        out_specs=VMEM,
        scratch_shapes=[pltpu.VMEM((prompts * TILE, lanes), f32)],
        name="chunk",
        compiler_params=limit(4),
    )(arrived, sums, stats)
    got = lax.all_to_all(chunk, "tp_0", split_axis=0, concat_axis=0, tiled=True)
    both = lax.all_gather(got, "tp_1", axis=0, tiled=True)

    turns_of = rings // 2
    y, k = np.divmod(np.arange(rings * count), count)
    tables = []
    for third in range(prompts // EXTRA):
        source = turns_of * (k - prompts) + (third - y) % turns_of
        extra = np.where(source < prompts, per_device * source + rings + y // turns_of, -1)
        tables.append(np.where(k < prompts, per_device * k + y, extra))
    keys, values, rope, attended = pl.pallas_call(
        finish_kernel,
        out_shape=(
            shaped((row_count, key_up_weight.shape[1])),
            shaped((row_count, value_up_weight.shape[1])),
            shaped((ROPE, row_count)),
            shaped((1, value_up_weight.shape[1])),
        ),
        in_specs=[VMEM, VMEM, HBM, VMEM, VMEM, VMEM],
        out_specs=(VMEM,) * 4,
        scratch_shapes=[
            pltpu.VMEM((rings * count, width), bf16),
            pltpu.VMEM((rings * count, ROPE), bf16),
            pltpu.VMEM(value_up_weight.shape, bf16),
            pltpu.SemaphoreType.DMA(()),
        ],
        name="finish",
        compiler_params=limit(8),
    )(
        both,
        key_up_weight,
        pinned(value_up_weight),
        query_nope,
        query_rope,
        jnp.asarray(np.stack(tables), jnp.int32),
    )
    return (keys[None], values[None], rope.T[None], attended)


def solution(mesh):
    split = Mesh(mesh.devices.reshape(mesh.shape["sp"], 8, 2), ("sp", "tp_0", "tp_1"))
    return jax.shard_map(
        on_device,
        mesh=split,
        in_specs=(
            P(None, "sp", TP),
            P(),
            P(),
            P(),
            P(None, TP),
            P(None, TP),
            P("sp", TP, None),
            P("sp", TP, None),
            P("sp", TP),
            P("sp", TP),
        ),
        out_specs=(P("sp", None, TP), P("sp", None, TP), P("sp", None, None), P("sp", TP)),
        check_vma=False,
    )
```

```python
import jax
import jax.numpy as jnp
import numpy as np
from jax import lax
from jax.experimental import pallas as pl
from jax.experimental.pallas import tpu as pltpu
from jax.sharding import Mesh
from jax.sharding import PartitionSpec as P

PLAIN_KEY_WIDTH = 128
ROPE = 64
VALUE_WIDTH = 128
PAST_POSITIONS = 32768
TP = ("tp_0", "tp_1")
EXTRA = 16
TILE = 8
FACTOR = (PLAIN_KEY_WIDTH + ROPE) ** (-0.5)

epsilon = 1e-06
rope_theta = 10000.0

VMEM = pl.BlockSpec(memory_space=pltpu.VMEM)
HBM = pl.BlockSpec(memory_space=pltpu.HBM)
MIB = 1 << 20
f32, bf16 = jnp.float32, jnp.bfloat16
NT = (((1,), (1,)), ((), ()))


def mm(a, b):
    return jnp.dot(a, b, preferred_element_type=f32)


def mm_nt(a, b):
    return lax.dot_general(a, b, NT, preferred_element_type=f32)


def iota(shape, dim):
    return lax.broadcasted_iota(jnp.int32, shape, dim)


def by_head(row, width):
    shape = (TILE, row.shape[1])
    spread = jnp.broadcast_to(row.astype(f32), shape)
    return jnp.where(iota(shape, 1) // width == iota(shape, 0), spread, 0.0).astype(bf16)


def three(x):
    high = x.astype(bf16).astype(f32)
    rest = x - high
    middle = rest.astype(bf16).astype(f32)
    return high, middle, rest - middle


def pack_kernel(
    tokens_hbm,
    nope_hbm,
    turn_hbm,
    key_hbm,
    angle_ref,
    out_ref,
    angle_out_ref,
    nope_ref,
    turn_ref,
    key_ref,
    sem,
):
    needed = [
        pltpu.make_async_copy(source, target, sem.at[k])
        for k, (source, target) in enumerate(
            ((key_hbm, key_ref), (nope_hbm, nope_ref), (turn_hbm, turn_ref))
        )
    ]
    for copy in needed:
        copy.start()
    angle_out_ref[...] = angle_ref[...]
    rings, lines, half = out_ref.shape
    prompts = tokens_hbm.shape[1]
    copies = [pltpu.make_async_copy(tokens_hbm.at[:rings], out_ref.at[:, :prompts], sem.at[3])]
    last = prompts // EXTRA - 1
    for y in range(rings):
        third = jnp.minimum(lax.rem(y % (rings // 2) + lax.axis_index("sp"), rings // 2), last)
        part = pl.ds(pl.multiple_of(third * EXTRA, EXTRA), EXTRA)
        source = tokens_hbm.at[rings + y // (rings // 2), part]
        target = out_ref.at[y, prompts : prompts + EXTRA]
        copies.append(pltpu.make_async_copy(source, target, sem.at[4 + y]))
    for copy in copies:
        copy.start()
    for copy in needed:
        copy.wait()
    latent = mm_nt(by_head(nope_ref[...], PLAIN_KEY_WIDTH), key_ref[...])
    turn = turn_ref[...].astype(f32)
    blank = jnp.zeros((1, half - ROPE), f32)
    query = [latent[0:2, :half], latent[0:2, half:]]
    query += [jnp.concatenate([turn[:, h * ROPE : (h + 1) * ROPE], blank], axis=1) for h in (0, 1)]
    query.append(jnp.zeros((2, half), f32))
    query = jnp.concatenate(query, axis=0).astype(bf16)
    for y in range(rings):
        out_ref[y, lines - TILE :, :] = query
    for copy in copies:
        copy.wait()


def project_kernel(
    rows_ref,
    angle_ref,
    cached_ref,
    past_ref,
    turn_down_hbm,
    gain_hbm,
    down_hbm,
    out_ref,
    sums_ref,
    stats_ref,
    line_ref,
    turn_down_ref,
    gain_ref,
    down_ref,
    sem,
):
    ranks, _, features = rows_ref.shape
    rings = ranks // 2
    prompts, tiles, lanes = out_ref.shape
    count = prompts + EXTRA
    width = down_ref.shape[1]
    copies = [
        pltpu.make_async_copy(turn_down_hbm, turn_down_ref, sem.at[0]),
        pltpu.make_async_copy(gain_hbm, gain_ref, sem.at[1]),
    ]
    for y in range(rings):
        part = pl.ds(2 * y * features, 2 * features)
        copies.append(pltpu.make_async_copy(down_hbm.at[part], down_ref.at[part], sem.at[2 + y]))
    for copy in copies:
        copy.start()
    line_ref[...] = jnp.zeros_like(line_ref)
    read_cached(rows_ref, cached_ref, past_ref, sums_ref, stats_ref)
    raw = jnp.zeros((count, width), f32)
    turned = jnp.zeros((count, ROPE), f32)
    copies[0].wait()
    copies[1].wait()
    for t in range(ranks):
        x = rows_ref[(t % 2) * rings + t // 2, :count, :]
        turned = turned + mm_nt(x, turn_down_ref[:, t * features : (t + 1) * features])
    for t in range(ranks):
        if t % 2 == 0:
            copies[2 + t // 2].wait()
        x = rows_ref[(t % 2) * rings + t // 2, :count, :]
        raw = raw + mm(x, down_ref[t * features : (t + 1) * features, :])
    scale = lax.rsqrt(jnp.mean(raw * raw, axis=-1, keepdims=True) + epsilon)
    latent = raw * scale * gain_ref[...]
    first, second = turned[:, : ROPE // 2], turned[:, ROPE // 2 :]
    full = iota((count, ROPE // 2), 0) < prompts
    cos = jnp.where(full, angle_ref[0, 0:1, :], angle_ref[0, 1:2, :])
    sin = jnp.where(full, angle_ref[1, 0:1, :], angle_ref[1, 1:2, :])
    turned = jnp.where(
        lax.axis_index("tp_1") == 0, first * cos - second * sin, first * sin + second * cos
    )
    half = width // 2
    own = jnp.where(lax.axis_index("tp_1") == 0, latent[:, :half], latent[:, half:])

    def repeated(x):
        return jnp.concatenate([x[prompts:]] * (prompts // EXTRA))

    parts = [own[:prompts, :lanes], own[:prompts, lanes:]]
    parts += [repeated(own[:, :lanes]), repeated(own[:, lanes:])]
    blank = jnp.zeros((prompts, lanes - ROPE), f32)
    parts.append(jnp.concatenate([turned[:prompts], repeated(turned), blank], axis=1))
    for k, part in enumerate(parts):
        line_ref[pl.ds(k, prompts, stride=tiles), :] = part
    out_ref[...] = line_ref[...].astype(bf16).reshape(out_ref.shape)


def read_cached(rows_ref, cached_ref, past_ref, sums_ref, stats_ref):
    ranks, count, features = rows_ref.shape
    rings = ranks // 2
    width = cached_ref.shape[1]
    heads = 2 * ranks
    group = heads // rings
    lines = rows_ref[:, count - TILE :, :].reshape(ranks * TILE, features)
    shape = (heads, ranks * TILE)
    head, line = iota(shape, 0), iota(shape, 1)
    source = ((head // 2) % 2) * rings + head // 4

    def pick(first):
        wanted = source * TILE + first + head % 2
        return mm(jnp.where(line == wanted, 1.0, 0.0).astype(bf16), lines).astype(bf16)

    query = jnp.concatenate([pick(0), pick(2)], axis=1)
    turn = pick(4)[:, :ROPE]
    cached = cached_ref[...]
    score = (mm_nt(query, cached) + mm(turn, past_ref[...])) * FACTOR
    peak = jnp.max(score, axis=-1, keepdims=True)
    weight = jnp.exp(score - peak)
    total = jnp.sum(weight, axis=-1, keepdims=True)
    summed = mm(weight.astype(bf16), cached)
    high = summed.astype(bf16).astype(f32)
    low = summed - high

    shape = (heads, width // 2)
    column = iota(shape, 1) // 8 - 6 * (iota(shape, 0) % group)
    spread = jnp.zeros(shape, f32)
    for k, part in enumerate((*three(peak), *three(total))):
        spread = jnp.where(column == k, part, spread)
    shape = (rings, heads)
    wanted = jnp.where(iota(shape, 0) == iota(shape, 1) // group, 1.0, 0.0)
    numbers = mm(wanted.astype(bf16), spread.astype(bf16))
    for y in range(rings):
        at = slice(group * y, group * (y + 1))
        sums_ref[y] = jnp.concatenate([high[at], low[at]]).astype(bf16)
    stats_ref[...] = numbers


def chunk_kernel(lines_ref, sums_ref, stats_ref, out_ref, flat_ref):
    prompts, tiles, lanes = lines_ref.shape
    rings, lines, width = out_ref.shape
    turns = rings // 2
    flat_ref[...] = lines_ref[...].reshape(prompts * tiles, lanes).astype(f32)
    first = lax.rem(lax.axis_index("sp") // EXTRA + rings - lax.axis_index("tp_0"), turns)

    def some(k):
        return flat_ref[pl.ds(first * tiles + k, prompts // turns, stride=turns * tiles), :]

    full = [flat_ref[pl.ds(k, prompts, stride=tiles), :] for k in (0, 1, 4)]
    spare = EXTRA - prompts // turns
    stacked = jnp.concatenate(
        [
            jnp.concatenate(full[:2], axis=1),
            jnp.concatenate([some(2), some(3)], axis=1),
            jnp.zeros((spare, width // 2), f32),
        ]
    )
    count = stacked.shape[0] // 2
    latent = jnp.concatenate([stacked[:count], stacked[count:]], axis=1).astype(bf16)
    half = ROPE // 2
    turned = jnp.concatenate(
        [full[2][:, :half], some(4)[:, half:ROPE], jnp.zeros((spare, half), f32)]
    )
    turned = jnp.concatenate(
        [turned[TILE * k : TILE * (k + 1)] for k in range(2 * count // TILE)], axis=1
    )
    for y in range(rings):
        out_ref[y, :count, :] = latent
        out_ref[y, count : count + TILE, :] = sums_ref[y]
        numbers = jnp.concatenate(
            [stats_ref[y : y + 1, :], jnp.zeros((TILE - 1, width // 2), f32)]
        )
        out_ref[y, count + TILE :, :] = jnp.concatenate([turned, numbers], axis=1).astype(bf16)


def finish_kernel(
    both_ref,
    key_ref,
    value_hbm,
    nope_ref,
    turn_ref,
    place_ref,
    keys_ref,
    values_ref,
    rope_ref,
    out_ref,
    latent_ref,
    turned_ref,
    value_ref,
    sem,
):
    load = pltpu.make_async_copy(value_hbm, value_ref, sem)
    load.start()
    sources, lines, width = both_ref.shape
    rings = sources // 2
    count = lines - 2 * TILE
    rows = keys_ref.shape[0]
    group = 4
    half = ROPE // 2
    for y in range(rings):
        halves = []
        for c in range(2):
            source = c * rings + y
            columns = slice(c * width // 2, (c + 1) * width // 2)
            for upper in range(2):
                at = slice((2 * y + upper) * count, (2 * y + upper + 1) * count)
                latent_ref[at, columns] = both_ref[
                    source, :count, upper * width // 2 : (upper + 1) * width // 2
                ]
            packed = both_ref[source, count + TILE :, :].astype(f32)
            halves.append(
                jnp.concatenate(
                    [packed[:, half * k : half * (k + 1)] for k in range(2 * count // TILE)]
                )
            )
        at = slice(2 * y * count, 2 * (y + 1) * count)
        turned_ref[at, :] = jnp.concatenate(halves, axis=1).astype(bf16)

    third = lax.axis_index("sp") // EXTRA
    place = place_ref[0:1, :]
    for k in range(1, place_ref.shape[0]):
        place = jnp.where(third == k, place_ref[k : k + 1, :], place)
    held = latent_ref.shape[0]
    move = jnp.where(iota((rows, held), 0) == place, 1.0, 0.0).astype(bf16)
    latent = mm(move, latent_ref[...]).astype(bf16)
    turned = mm(move, turned_ref[...]).astype(bf16)
    keys = mm(latent, key_ref[...]).astype(bf16)
    keys_ref[...] = keys
    load.wait()
    values = mm(latent, value_ref[...]).astype(bf16)
    values_ref[...] = values
    same = jnp.where(iota((ROPE, ROPE), 0) == iota((ROPE, ROPE), 1), 1.0, 0.0).astype(bf16)
    rope = mm_nt(same, turned).astype(bf16)
    rope_ref[...] = rope

    nope = by_head(nope_ref[...], PLAIN_KEY_WIDTH)
    turn = by_head(turn_ref[...], ROPE)
    score = (mm_nt(nope, keys) + mm(turn, jnp.concatenate([rope, rope], axis=0))) * FACTOR

    shape = (group, width // 2)
    place = iota(shape, 1) // 8 - 6 * iota(shape, 0)
    mine = [(iota(shape, 1) % 8 == 0) & (place >= k) & (place < k + 3) for k in (0, 3)]
    peaks, totals = [], []
    for source in range(sources):
        numbers = both_ref[source, count + TILE :, width // 2 :].astype(f32)[:1]
        for found, where in zip((peaks, totals), mine):
            found.append(jnp.sum(jnp.where(where, numbers, 0.0), axis=-1, keepdims=True))
    past_peak = peaks[0]
    for x in peaks[1:]:
        past_peak = jnp.maximum(past_peak, x)
    past_total = jnp.zeros((group, 1), f32)
    past_sum = jnp.zeros((TILE, width), f32)
    for k in range(sources):
        share = jnp.exp(peaks[k] - past_peak)
        past_total = past_total + totals[k] * share
        sums = both_ref[k, count : count + TILE, :].astype(f32)
        past_sum = past_sum + sums * jnp.concatenate([share, share])
    past_sum = past_sum[:group] + past_sum[group:]

    def own(x):
        half = group // 2
        mine = jnp.where(lax.axis_index("tp_1") == 0, x[:half], x[half:])
        return jnp.concatenate([mine, jnp.zeros((TILE - half, x.shape[1]), f32)])

    past_peak, past_total, past_sum = own(past_peak), own(past_total), own(past_sum)
    peak = jnp.maximum(past_peak, jnp.max(score, axis=-1, keepdims=True))
    share = jnp.exp(past_peak - peak)
    weight = jnp.exp(score - peak)
    denominator = past_total * share + jnp.sum(weight, axis=-1, keepdims=True)
    result = mm((past_sum * share).astype(bf16), value_ref[...]) + mm(weight.astype(bf16), values)
    result = result / denominator
    shape = result.shape
    result = jnp.where(iota(shape, 1) // VALUE_WIDTH == iota(shape, 0), result, 0.0)
    out_ref[...] = jnp.sum(result, axis=0, keepdims=True).astype(bf16)


def shaped(shape, dtype=bf16):
    return jax.ShapeDtypeStruct(shape, dtype)


def limit(mib):
    return pltpu.CompilerParams(vmem_limit_bytes=mib * MIB)


def pinned(x):
    return pltpu.with_memory_space_constraint(x, pltpu.HBM)


def on_device(
    tokens,
    latent_down_weight,
    w_rope_key,
    latent_norm_gain,
    key_up_weight,
    value_up_weight,
    cached_latent_rows,
    past_rope,
    query_nope,
    query_rope,
):
    prompts, per_device, features = tokens.shape
    width = latent_down_weight.shape[1]
    row_count = prompts * per_device
    rings = lax.axis_size("tp_0")
    ring = lax.axis_index("tp_0")
    device = lax.axis_index("sp")

    places = jnp.stack([ring, rings + ring // (rings // 2)])
    positions = (PAST_POSITIONS + device * per_device + places).astype(f32)
    halfway = ROPE // 2
    frequency = rope_theta ** (-jnp.arange(halfway, dtype=f32) / halfway)
    angles = positions[:, None] * frequency

    turns = jnp.stack([jnp.cos(angles), jnp.sin(angles)])
    sources = (query_nope, query_rope, key_up_weight)
    outgoing, turns = pl.pallas_call(
        pack_kernel,
        out_shape=(shaped((rings, prompts + EXTRA + TILE, features)), shaped(turns.shape, f32)),
        in_specs=[HBM] * 4 + [VMEM],
        out_specs=(VMEM, VMEM),
        scratch_shapes=[pltpu.VMEM(x.shape, bf16) for x in sources]
        + [pltpu.SemaphoreType.DMA((4 + rings,))],
        name="pack",
        compiler_params=limit(4),
    )(pinned(tokens.transpose(1, 0, 2)), *(pinned(x) for x in sources), turns)
    rows = lax.all_to_all(outgoing, "tp_0", split_axis=0, concat_axis=0, tiled=True)
    rows = lax.all_gather(rows, "tp_1", axis=0, tiled=True)

    lanes = 128
    sources = (w_rope_key.T, latent_norm_gain[None], latent_down_weight)
    lines, sums, stats = pl.pallas_call(
        project_kernel,
        out_shape=(
            shaped((prompts, TILE, lanes)),
            shaped((rings, TILE, width)),
            shaped((rings, width // 2), f32),
        ),
        in_specs=[VMEM] * 4 + [HBM] * 3,
        out_specs=(VMEM,) * 3,
        scratch_shapes=[pltpu.VMEM((prompts * TILE, lanes), f32)]
        + [pltpu.VMEM(x.shape, x.dtype) for x in sources]
        + [pltpu.SemaphoreType.DMA((rings + 2,))],
        name="project",
        compiler_params=limit(12),
    )(rows, turns, cached_latent_rows[0], past_rope[0].T, *(pinned(x) for x in sources))
    arrived = lax.all_to_all(lines, "sp", split_axis=0, concat_axis=0, tiled=True)

    count = prompts + EXTRA
    chunk = pl.pallas_call(
        chunk_kernel,
        out_shape=shaped((rings, count // 2 + 2 * TILE, width)),
        in_specs=[VMEM] * 3,
        out_specs=VMEM,
        scratch_shapes=[pltpu.VMEM((prompts * TILE, lanes), f32)],
        name="chunk",
        compiler_params=limit(4),
    )(arrived, sums, stats)
    got = lax.all_to_all(chunk, "tp_0", split_axis=0, concat_axis=0, tiled=True)
    both = lax.all_gather(got, "tp_1", axis=0, tiled=True)

    turns_of = rings // 2
    y, k = np.divmod(np.arange(rings * count), count)
    tables = []
    for third in range(prompts // EXTRA):
        source = turns_of * (k - prompts) + (third - y) % turns_of
        extra = np.where(source < prompts, per_device * source + rings + y // turns_of, -1)
        tables.append(np.where(k < prompts, per_device * k + y, extra))
    keys, values, rope, attended = pl.pallas_call(
        finish_kernel,
        out_shape=(
            shaped((row_count, key_up_weight.shape[1])),
            shaped((row_count, value_up_weight.shape[1])),
            shaped((ROPE, row_count)),
            shaped((1, value_up_weight.shape[1])),
        ),
        in_specs=[VMEM, VMEM, HBM, VMEM, VMEM, VMEM],
        out_specs=(VMEM,) * 4,
        scratch_shapes=[
            pltpu.VMEM((rings * count, width), bf16),
            pltpu.VMEM((rings * count, ROPE), bf16),
            pltpu.VMEM(value_up_weight.shape, bf16),
            pltpu.SemaphoreType.DMA(()),
        ],
        name="finish",
        compiler_params=limit(8),
    )(
        both,
        key_up_weight,
        pinned(value_up_weight),
        query_nope,
        query_rope,
        jnp.asarray(np.stack(tables), jnp.int32),
    )
    return (keys[None], values[None], rope.T[None], attended)


def solution(mesh):
    split = Mesh(mesh.devices.reshape(mesh.shape["sp"], 8, 2), ("sp", "tp_0", "tp_1"))
    return jax.shard_map(
        on_device,
        mesh=split,
        in_specs=(
            P(None, "sp", TP),
            P(),
            P(),
            P(),
            P(None, TP),
            P(None, TP),
            P("sp", TP, None),
            P("sp", TP, None),
            P("sp", TP),
            P("sp", TP),
        ),
        out_specs=(P("sp", None, TP), P("sp", None, TP), P("sp", None, None), P("sp", TP)),
        check_vma=False,
    )
```

```python
import jax
import jax.numpy as jnp
import numpy as np
from jax import lax
from jax.experimental import pallas as pl
from jax.experimental.pallas import tpu as pltpu
from jax.sharding import Mesh
from jax.sharding import PartitionSpec as P

PLAIN_KEY_WIDTH = 128
ROPE = 64
VALUE_WIDTH = 128
PAST_POSITIONS = 32768
TP = ("tp_0", "tp_1")
EXTRA = 16
TILE = 8
FACTOR = (PLAIN_KEY_WIDTH + ROPE) ** (-0.5)

epsilon = 1e-06
rope_theta = 10000.0

VMEM = pl.BlockSpec(memory_space=pltpu.VMEM)
HBM = pl.BlockSpec(memory_space=pltpu.HBM)
ANY = pl.BlockSpec(memory_space=pl.ANY)
MIB = 1 << 20
f32, bf16 = jnp.float32, jnp.bfloat16
NT = (((1,), (1,)), ((), ()))


def mm(a, b):
    return jnp.dot(a, b, preferred_element_type=f32)


def mm_nt(a, b):
    return lax.dot_general(a, b, NT, preferred_element_type=f32)


def iota(shape, dim):
    return lax.broadcasted_iota(jnp.int32, shape, dim)


def by_head(row, width):
    shape = (TILE, row.shape[1])
    spread = jnp.broadcast_to(row.astype(f32), shape)
    return jnp.where(iota(shape, 1) // width == iota(shape, 0), spread, 0.0).astype(bf16)


def three(x):
    high = x.astype(bf16).astype(f32)
    rest = x - high
    middle = rest.astype(bf16).astype(f32)
    return high, middle, rest - middle


def pack_kernel(
    tokens_hbm,
    nope_hbm,
    turn_hbm,
    key_hbm,
    cached_hbm,
    past_hbm,
    angle_ref,
    out_ref,
    angle_out_ref,
    cached_ref,
    past_ref,
    nope_ref,
    turn_ref,
    key_ref,
    sem,
):
    needed = [
        pltpu.make_async_copy(source, target, sem.at[k])
        for k, (source, target) in enumerate(
            ((key_hbm, key_ref), (nope_hbm, nope_ref), (turn_hbm, turn_ref))
        )
    ]
    for copy in needed:
        copy.start()
    angle_out_ref[...] = angle_ref[...]
    rings, lines, half = out_ref.shape
    prompts = tokens_hbm.shape[1]
    copies = [pltpu.make_async_copy(tokens_hbm.at[:rings], out_ref.at[:, :prompts], sem.at[3])]
    last = prompts // EXTRA - 1
    for y in range(rings):
        third = jnp.minimum(lax.rem(y % (rings // 2) + lax.axis_index("sp"), rings // 2), last)
        part = pl.ds(pl.multiple_of(third * EXTRA, EXTRA), EXTRA)
        source = tokens_hbm.at[rings + y // (rings // 2), part]
        target = out_ref.at[y, prompts : prompts + EXTRA]
        copies.append(pltpu.make_async_copy(source, target, sem.at[4 + y]))
    copies.append(pltpu.make_async_copy(past_hbm, past_ref, sem.at[4 + rings]))
    copies.append(pltpu.make_async_copy(cached_hbm, cached_ref, sem.at[5 + rings]))
    for copy in copies:
        copy.start()
    for copy in needed:
        copy.wait()
    latent = mm_nt(by_head(nope_ref[...], PLAIN_KEY_WIDTH), key_ref[...])
    turn = turn_ref[...].astype(f32)
    blank = jnp.zeros((1, half - ROPE), f32)
    query = [latent[0:2, :half], latent[0:2, half:]]
    query += [jnp.concatenate([turn[:, h * ROPE : (h + 1) * ROPE], blank], axis=1) for h in (0, 1)]
    query.append(jnp.zeros((2, half), f32))
    query = jnp.concatenate(query, axis=0).astype(bf16)
    for y in range(rings):
        out_ref[y, lines - TILE :, :] = query
    for copy in copies:
        copy.wait()


def project_kernel(
    rows_ref,
    angle_ref,
    cached_ref,
    past_ref,
    turn_down_hbm,
    gain_hbm,
    down_hbm,
    out_ref,
    sums_ref,
    stats_ref,
    line_ref,
    turn_down_ref,
    gain_ref,
    down_ref,
    sem,
):
    ranks, _, features = rows_ref.shape
    rings = ranks // 2
    prompts, tiles, lanes = out_ref.shape
    count = prompts + EXTRA
    width = down_ref.shape[1]
    copies = [
        pltpu.make_async_copy(turn_down_hbm, turn_down_ref, sem.at[0]),
        pltpu.make_async_copy(gain_hbm, gain_ref, sem.at[1]),
    ]
    for y in range(rings):
        part = pl.ds(2 * y * features, 2 * features)
        copies.append(pltpu.make_async_copy(down_hbm.at[part], down_ref.at[part], sem.at[2 + y]))
    for copy in copies:
        copy.start()
    line_ref[...] = jnp.zeros_like(line_ref)
    read_cached(rows_ref, cached_ref, past_ref, sums_ref, stats_ref)
    raw = jnp.zeros((count, width), f32)
    turned = jnp.zeros((count, ROPE), f32)
    copies[0].wait()
    copies[1].wait()
    for t in range(ranks):
        x = rows_ref[(t % 2) * rings + t // 2, :count, :]
        turned = turned + mm_nt(x, turn_down_ref[:, t * features : (t + 1) * features])
    for t in range(ranks):
        if t % 2 == 0:
            copies[2 + t // 2].wait()
        x = rows_ref[(t % 2) * rings + t // 2, :count, :]
        raw = raw + mm(x, down_ref[t * features : (t + 1) * features, :])
    scale = lax.rsqrt(jnp.mean(raw * raw, axis=-1, keepdims=True) + epsilon)
    latent = raw * scale * gain_ref[...]
    first, second = turned[:, : ROPE // 2], turned[:, ROPE // 2 :]
    full = iota((count, ROPE // 2), 0) < prompts
    cos = jnp.where(full, angle_ref[0, 0:1, :], angle_ref[0, 1:2, :])
    sin = jnp.where(full, angle_ref[1, 0:1, :], angle_ref[1, 1:2, :])
    turned = jnp.where(
        lax.axis_index("tp_1") == 0, first * cos - second * sin, first * sin + second * cos
    )
    half = width // 2
    own = jnp.where(lax.axis_index("tp_1") == 0, latent[:, :half], latent[:, half:])

    def repeated(x):
        return jnp.concatenate([x[prompts:]] * (prompts // EXTRA))

    parts = [own[:prompts, :lanes], own[:prompts, lanes:]]
    parts += [repeated(own[:, :lanes]), repeated(own[:, lanes:])]
    blank = jnp.zeros((prompts, lanes - ROPE), f32)
    parts.append(jnp.concatenate([turned[:prompts], repeated(turned), blank], axis=1))
    for k, part in enumerate(parts):
        line_ref[pl.ds(k, prompts, stride=tiles), :] = part
    out_ref[...] = line_ref[...].astype(bf16).reshape(out_ref.shape)


def read_cached(rows_ref, cached_ref, past_ref, sums_ref, stats_ref):
    ranks, count, features = rows_ref.shape
    rings = ranks // 2
    width = cached_ref.shape[1]
    heads = 2 * ranks
    group = heads // rings
    lines = rows_ref[:, count - TILE :, :].reshape(ranks * TILE, features)
    shape = (heads, ranks * TILE)
    head, line = iota(shape, 0), iota(shape, 1)
    source = ((head // 2) % 2) * rings + head // 4

    def pick(first):
        wanted = source * TILE + first + head % 2
        return mm(jnp.where(line == wanted, 1.0, 0.0).astype(bf16), lines).astype(bf16)

    query = jnp.concatenate([pick(0), pick(2)], axis=1)
    turn = pick(4)[:, :ROPE]
    cached = cached_ref[...]
    score = (mm_nt(query, cached) + mm(turn, past_ref[...])) * FACTOR
    peak = jnp.max(score, axis=-1, keepdims=True)
    weight = jnp.exp(score - peak)
    total = jnp.sum(weight, axis=-1, keepdims=True)
    summed = mm(weight.astype(bf16), cached)
    high = summed.astype(bf16).astype(f32)
    low = summed - high

    shape = (heads, width // 2)
    column = iota(shape, 1) // 8 - 6 * (iota(shape, 0) % group)
    spread = jnp.zeros(shape, f32)
    for k, part in enumerate((*three(peak), *three(total))):
        spread = jnp.where(column == k, part, spread)
    shape = (rings, heads)
    wanted = jnp.where(iota(shape, 0) == iota(shape, 1) // group, 1.0, 0.0)
    numbers = mm(wanted.astype(bf16), spread.astype(bf16))
    for y in range(rings):
        at = slice(group * y, group * (y + 1))
        sums_ref[y] = jnp.concatenate([high[at], low[at]]).astype(bf16)
    stats_ref[...] = numbers


def chunk_kernel(lines_ref, sums_ref, stats_ref, out_ref, flat_ref):
    prompts, tiles, lanes = lines_ref.shape
    rings, lines, width = out_ref.shape
    turns = rings // 2
    flat_ref[...] = lines_ref[...].reshape(prompts * tiles, lanes).astype(f32)
    first = lax.rem(lax.axis_index("sp") // EXTRA + rings - lax.axis_index("tp_0"), turns)

    def some(k):
        return flat_ref[pl.ds(first * tiles + k, prompts // turns, stride=turns * tiles), :]

    full = [flat_ref[pl.ds(k, prompts, stride=tiles), :] for k in (0, 1, 4)]
    spare = EXTRA - prompts // turns
    stacked = jnp.concatenate(
        [
            jnp.concatenate(full[:2], axis=1),
            jnp.concatenate([some(2), some(3)], axis=1),
            jnp.zeros((spare, width // 2), f32),
        ]
    )
    count = stacked.shape[0] // 2
    latent = jnp.concatenate([stacked[:count], stacked[count:]], axis=1).astype(bf16)
    half = ROPE // 2
    turned = jnp.concatenate(
        [full[2][:, :half], some(4)[:, half:ROPE], jnp.zeros((spare, half), f32)]
    )
    turned = jnp.concatenate(
        [turned[TILE * k : TILE * (k + 1)] for k in range(2 * count // TILE)], axis=1
    )
    for y in range(rings):
        out_ref[y, :count, :] = latent
        out_ref[y, count : count + TILE, :] = sums_ref[y]
        numbers = jnp.concatenate(
            [stats_ref[y : y + 1, :], jnp.zeros((TILE - 1, width // 2), f32)]
        )
        out_ref[y, count + TILE :, :] = jnp.concatenate([turned, numbers], axis=1).astype(bf16)


def finish_kernel(
    both_ref,
    key_ref,
    value_hbm,
    nope_ref,
    turn_ref,
    place_ref,
    keys_ref,
    values_ref,
    rope_ref,
    out_ref,
    latent_ref,
    turned_ref,
    value_ref,
    sem,
):
    load = pltpu.make_async_copy(value_hbm, value_ref, sem)
    load.start()
    sources, lines, width = both_ref.shape
    rings = sources // 2
    count = lines - 2 * TILE
    rows = keys_ref.shape[0]
    group = 4
    half = ROPE // 2
    for y in range(rings):
        halves = []
        for c in range(2):
            source = c * rings + y
            columns = slice(c * width // 2, (c + 1) * width // 2)
            for upper in range(2):
                at = slice((2 * y + upper) * count, (2 * y + upper + 1) * count)
                latent_ref[at, columns] = both_ref[
                    source, :count, upper * width // 2 : (upper + 1) * width // 2
                ]
            packed = both_ref[source, count + TILE :, :].astype(f32)
            halves.append(
                jnp.concatenate(
                    [packed[:, half * k : half * (k + 1)] for k in range(2 * count // TILE)]
                )
            )
        at = slice(2 * y * count, 2 * (y + 1) * count)
        turned_ref[at, :] = jnp.concatenate(halves, axis=1).astype(bf16)

    third = lax.axis_index("sp") // EXTRA
    place = place_ref[0:1, :]
    for k in range(1, place_ref.shape[0]):
        place = jnp.where(third == k, place_ref[k : k + 1, :], place)
    held = latent_ref.shape[0]
    move = jnp.where(iota((rows, held), 0) == place, 1.0, 0.0).astype(bf16)
    latent = mm(move, latent_ref[...]).astype(bf16)
    turned = mm(move, turned_ref[...]).astype(bf16)
    keys = mm(latent, key_ref[...]).astype(bf16)
    keys_ref[...] = keys
    load.wait()
    values = mm(latent, value_ref[...]).astype(bf16)
    values_ref[...] = values
    same = jnp.where(iota((ROPE, ROPE), 0) == iota((ROPE, ROPE), 1), 1.0, 0.0).astype(bf16)
    rope = mm_nt(same, turned).astype(bf16)
    rope_ref[...] = rope

    nope = by_head(nope_ref[...], PLAIN_KEY_WIDTH)
    turn = by_head(turn_ref[...], ROPE)
    score = (mm_nt(nope, keys) + mm(turn, jnp.concatenate([rope, rope], axis=0))) * FACTOR

    shape = (group, width // 2)
    place = iota(shape, 1) // 8 - 6 * iota(shape, 0)
    mine = [(iota(shape, 1) % 8 == 0) & (place >= k) & (place < k + 3) for k in (0, 3)]
    peaks, totals = [], []
    for source in range(sources):
        numbers = both_ref[source, count + TILE :, width // 2 :].astype(f32)[:1]
        for found, where in zip((peaks, totals), mine):
            found.append(jnp.sum(jnp.where(where, numbers, 0.0), axis=-1, keepdims=True))
    past_peak = peaks[0]
    for x in peaks[1:]:
        past_peak = jnp.maximum(past_peak, x)
    past_total = jnp.zeros((group, 1), f32)
    past_sum = jnp.zeros((TILE, width), f32)
    for k in range(sources):
        share = jnp.exp(peaks[k] - past_peak)
        past_total = past_total + totals[k] * share
        sums = both_ref[k, count : count + TILE, :].astype(f32)
        past_sum = past_sum + sums * jnp.concatenate([share, share])
    past_sum = past_sum[:group] + past_sum[group:]

    def own(x):
        half = group // 2
        mine = jnp.where(lax.axis_index("tp_1") == 0, x[:half], x[half:])
        return jnp.concatenate([mine, jnp.zeros((TILE - half, x.shape[1]), f32)])

    past_peak, past_total, past_sum = own(past_peak), own(past_total), own(past_sum)
    peak = jnp.maximum(past_peak, jnp.max(score, axis=-1, keepdims=True))
    share = jnp.exp(past_peak - peak)
    weight = jnp.exp(score - peak)
    denominator = past_total * share + jnp.sum(weight, axis=-1, keepdims=True)
    result = mm((past_sum * share).astype(bf16), value_ref[...]) + mm(weight.astype(bf16), values)
    result = result / denominator
    shape = result.shape
    result = jnp.where(iota(shape, 1) // VALUE_WIDTH == iota(shape, 0), result, 0.0)
    out_ref[...] = jnp.sum(result, axis=0, keepdims=True).astype(bf16)


def shaped(shape, dtype=bf16):
    return jax.ShapeDtypeStruct(shape, dtype)


def limit(mib):
    return pltpu.CompilerParams(vmem_limit_bytes=mib * MIB)


def pinned(x):
    return pltpu.with_memory_space_constraint(x, pltpu.HBM)


def on_device(
    tokens,
    latent_down_weight,
    w_rope_key,
    latent_norm_gain,
    key_up_weight,
    value_up_weight,
    cached_latent_rows,
    past_rope,
    query_nope,
    query_rope,
):
    prompts, per_device, features = tokens.shape
    width = latent_down_weight.shape[1]
    row_count = prompts * per_device
    rings = lax.axis_size("tp_0")
    ring = lax.axis_index("tp_0")
    device = lax.axis_index("sp")

    places = jnp.stack([ring, rings + ring // (rings // 2)])
    positions = (PAST_POSITIONS + device * per_device + places).astype(f32)
    halfway = ROPE // 2
    frequency = rope_theta ** (-jnp.arange(halfway, dtype=f32) / halfway)
    angles = positions[:, None] * frequency

    turns = jnp.stack([jnp.cos(angles), jnp.sin(angles)])
    sources = (query_nope, query_rope, key_up_weight)
    past = (cached_latent_rows[0], past_rope[0].T)
    outgoing, turns, *past = pl.pallas_call(
        pack_kernel,
        out_shape=(
            shaped((rings, prompts + EXTRA + TILE, features)),
            shaped(turns.shape, f32),
            *(shaped(x.shape) for x in past),
        ),
        in_specs=[HBM] * 6 + [VMEM],
        out_specs=(VMEM, VMEM, ANY, ANY),
        scratch_shapes=[pltpu.VMEM(x.shape, bf16) for x in sources]
        + [pltpu.SemaphoreType.DMA((6 + rings,))],
        name="pack",
        compiler_params=limit(4),
    )(*(pinned(x) for x in (tokens.transpose(1, 0, 2), *sources, *past)), turns)
    rows = lax.all_to_all(outgoing, "tp_0", split_axis=0, concat_axis=0, tiled=True)
    rows = lax.all_gather(rows, "tp_1", axis=0, tiled=True)

    lanes = 128
    sources = (w_rope_key.T, latent_norm_gain[None], latent_down_weight)
    lines, sums, stats = pl.pallas_call(
        project_kernel,
        out_shape=(
            shaped((prompts, TILE, lanes)),
            shaped((rings, TILE, width)),
            shaped((rings, width // 2), f32),
        ),
        in_specs=[VMEM] * 4 + [HBM] * 3,
        out_specs=(VMEM,) * 3,
        scratch_shapes=[pltpu.VMEM((prompts * TILE, lanes), f32)]
        + [pltpu.VMEM(x.shape, x.dtype) for x in sources]
        + [pltpu.SemaphoreType.DMA((rings + 2,))],
        name="project",
        compiler_params=limit(12),
    )(rows, turns, *past, *(pinned(x) for x in sources))
    arrived = lax.all_to_all(lines, "sp", split_axis=0, concat_axis=0, tiled=True)

    count = prompts + EXTRA
    chunk = pl.pallas_call(
        chunk_kernel,
        out_shape=shaped((rings, count // 2 + 2 * TILE, width)),
        in_specs=[VMEM] * 3,
        out_specs=VMEM,
        scratch_shapes=[pltpu.VMEM((prompts * TILE, lanes), f32)],
        name="chunk",
        compiler_params=limit(4),
    )(arrived, sums, stats)
    got = lax.all_to_all(chunk, "tp_0", split_axis=0, concat_axis=0, tiled=True)
    both = lax.all_gather(got, "tp_1", axis=0, tiled=True)

    turns_of = rings // 2
    y, k = np.divmod(np.arange(rings * count), count)
    tables = []
    for third in range(prompts // EXTRA):
        source = turns_of * (k - prompts) + (third - y) % turns_of
        extra = np.where(source < prompts, per_device * source + rings + y // turns_of, -1)
        tables.append(np.where(k < prompts, per_device * k + y, extra))
    keys, values, rope, attended = pl.pallas_call(
        finish_kernel,
        out_shape=(
            shaped((row_count, key_up_weight.shape[1])),
            shaped((row_count, value_up_weight.shape[1])),
            shaped((ROPE, row_count)),
            shaped((1, value_up_weight.shape[1])),
        ),
        in_specs=[VMEM, VMEM, HBM, VMEM, VMEM, VMEM],
        out_specs=(VMEM,) * 4,
        scratch_shapes=[
            pltpu.VMEM((rings * count, width), bf16),
            pltpu.VMEM((rings * count, ROPE), bf16),
            pltpu.VMEM(value_up_weight.shape, bf16),
            pltpu.SemaphoreType.DMA(()),
        ],
        name="finish",
        compiler_params=limit(8),
    )(
        both,
        key_up_weight,
        pinned(value_up_weight),
        query_nope,
        query_rope,
        jnp.asarray(np.stack(tables), jnp.int32),
    )
    return (keys[None], values[None], rope.T[None], attended)


def solution(mesh):
    split = Mesh(mesh.devices.reshape(mesh.shape["sp"], 8, 2), ("sp", "tp_0", "tp_1"))
    return jax.shard_map(
        on_device,
        mesh=split,
        in_specs=(
            P(None, "sp", TP),
            P(),
            P(),
            P(),
            P(None, TP),
            P(None, TP),
            P("sp", TP, None),
            P("sp", TP, None),
            P("sp", TP),
            P("sp", TP),
        ),
        out_specs=(P("sp", None, TP), P("sp", None, TP), P("sp", None, None), P("sp", TP)),
        check_vma=False,
    )
```

```python
import jax
import jax.numpy as jnp
import numpy as np
from jax import lax
from jax.experimental import pallas as pl
from jax.experimental.pallas import tpu as pltpu
from jax.sharding import Mesh
from jax.sharding import PartitionSpec as P

PLAIN_KEY_WIDTH = 128
ROPE = 64
VALUE_WIDTH = 128
PAST_POSITIONS = 32768
TP = ("tp_0", "tp_1")
EXTRA = 16
TILE = 8
FACTOR = (PLAIN_KEY_WIDTH + ROPE) ** (-0.5)

epsilon = 1e-06
rope_theta = 10000.0

VMEM = pl.BlockSpec(memory_space=pltpu.VMEM)
HBM = pl.BlockSpec(memory_space=pltpu.HBM)
ANY = pl.BlockSpec(memory_space=pl.ANY)
MIB = 1 << 20
f32, bf16 = jnp.float32, jnp.bfloat16
NT = (((1,), (1,)), ((), ()))


def mm(a, b):
    return jnp.dot(a, b, preferred_element_type=f32)


def mm_nt(a, b):
    return lax.dot_general(a, b, NT, preferred_element_type=f32)


def iota(shape, dim):
    return lax.broadcasted_iota(jnp.int32, shape, dim)


def by_head(row, width):
    shape = (TILE, row.shape[1])
    spread = jnp.broadcast_to(row.astype(f32), shape)
    return jnp.where(iota(shape, 1) // width == iota(shape, 0), spread, 0.0).astype(bf16)


def three(x):
    high = x.astype(bf16).astype(f32)
    rest = x - high
    middle = rest.astype(bf16).astype(f32)
    return high, middle, rest - middle


def pack_kernel(
    tokens_hbm,
    nope_hbm,
    turn_hbm,
    key_hbm,
    cached_hbm,
    past_hbm,
    angle_ref,
    out_ref,
    angle_out_ref,
    cached_ref,
    past_ref,
    nope_ref,
    turn_ref,
    key_ref,
    sem,
):
    needed = [
        pltpu.make_async_copy(source, target, sem.at[k])
        for k, (source, target) in enumerate(
            ((key_hbm, key_ref), (nope_hbm, nope_ref), (turn_hbm, turn_ref))
        )
    ]
    for copy in needed:
        copy.start()
    angle_out_ref[...] = angle_ref[...]
    rings, lines, half = out_ref.shape
    prompts = tokens_hbm.shape[1]
    copies = [pltpu.make_async_copy(tokens_hbm.at[:rings], out_ref.at[:, :prompts], sem.at[3])]
    last = prompts // EXTRA - 1
    for y in range(rings):
        third = jnp.minimum(lax.rem(y % (rings // 2) + lax.axis_index("sp"), rings // 2), last)
        part = pl.ds(pl.multiple_of(third * EXTRA, EXTRA), EXTRA)
        source = tokens_hbm.at[rings + y // (rings // 2), part]
        target = out_ref.at[y, prompts : prompts + EXTRA]
        copies.append(pltpu.make_async_copy(source, target, sem.at[4 + y]))
    copies.append(pltpu.make_async_copy(past_hbm, past_ref, sem.at[4 + rings]))
    copies.append(pltpu.make_async_copy(cached_hbm, cached_ref, sem.at[5 + rings]))
    for copy in copies:
        copy.start()
    for copy in needed:
        copy.wait()
    latent = mm_nt(by_head(nope_ref[...], PLAIN_KEY_WIDTH), key_ref[...])
    turn = turn_ref[...].astype(f32)
    blank = jnp.zeros((1, half - ROPE), f32)
    query = [latent[0:2, :half], latent[0:2, half:]]
    query += [jnp.concatenate([turn[:, h * ROPE : (h + 1) * ROPE], blank], axis=1) for h in (0, 1)]
    query.append(jnp.zeros((2, half), f32))
    query = jnp.concatenate(query, axis=0).astype(bf16)
    for y in range(rings):
        out_ref[y, lines - TILE :, :] = query
    for copy in copies:
        copy.wait()


def project_kernel(
    rows_ref,
    angle_ref,
    cached_ref,
    past_ref,
    turn_down_hbm,
    gain_hbm,
    down_hbm,
    out_ref,
    sums_ref,
    stats_ref,
    line_ref,
    turn_down_ref,
    gain_ref,
    down_ref,
    sem,
):
    ranks, _, features = rows_ref.shape
    rings = ranks // 2
    prompts, tiles, lanes = out_ref.shape
    count = prompts + EXTRA
    width = down_ref.shape[1]
    copies = [
        pltpu.make_async_copy(turn_down_hbm, turn_down_ref, sem.at[0]),
        pltpu.make_async_copy(gain_hbm, gain_ref, sem.at[1]),
    ]
    for y in range(rings):
        part = pl.ds(2 * y * features, 2 * features)
        copies.append(pltpu.make_async_copy(down_hbm.at[part], down_ref.at[part], sem.at[2 + y]))
    for copy in copies:
        copy.start()
    line_ref[...] = jnp.zeros_like(line_ref)
    read_cached(rows_ref, cached_ref, past_ref, sums_ref, stats_ref)
    raw = jnp.zeros((count, width), f32)
    turned = jnp.zeros((count, ROPE), f32)
    copies[0].wait()
    copies[1].wait()
    for t in range(ranks):
        x = rows_ref[(t % 2) * rings + t // 2, :count, :]
        turned = turned + mm_nt(x, turn_down_ref[:, t * features : (t + 1) * features])
    for t in range(ranks):
        if t % 2 == 0:
            copies[2 + t // 2].wait()
        x = rows_ref[(t % 2) * rings + t // 2, :count, :]
        raw = raw + mm(x, down_ref[t * features : (t + 1) * features, :])
    scale = lax.rsqrt(jnp.mean(raw * raw, axis=-1, keepdims=True) + epsilon)
    latent = raw * scale * gain_ref[...]
    first, second = turned[:, : ROPE // 2], turned[:, ROPE // 2 :]
    full = iota((count, ROPE // 2), 0) < prompts
    cos = jnp.where(full, angle_ref[0, 0:1, :], angle_ref[0, 1:2, :])
    sin = jnp.where(full, angle_ref[1, 0:1, :], angle_ref[1, 1:2, :])
    turned = jnp.where(
        lax.axis_index("tp_1") == 0, first * cos - second * sin, first * sin + second * cos
    )
    half = width // 2
    own = jnp.where(lax.axis_index("tp_1") == 0, latent[:, :half], latent[:, half:])

    def repeated(x):
        return jnp.concatenate([x[prompts:]] * (prompts // EXTRA))

    parts = [own[:prompts, :lanes], own[:prompts, lanes:]]
    parts += [repeated(own[:, :lanes]), repeated(own[:, lanes:])]
    blank = jnp.zeros((prompts, lanes - ROPE), f32)
    parts.append(jnp.concatenate([turned[:prompts], repeated(turned), blank], axis=1))
    for k, part in enumerate(parts):
        line_ref[pl.ds(k, prompts, stride=tiles), :] = part
    out_ref[...] = line_ref[...].astype(bf16).reshape(out_ref.shape)


def read_cached(rows_ref, cached_ref, past_ref, sums_ref, stats_ref):
    ranks, count, features = rows_ref.shape
    rings = ranks // 2
    heads = 2 * ranks
    lines = rows_ref[:, count - TILE :, :].reshape(ranks * TILE, features)
    shape = (heads, ranks * TILE)
    head, line = iota(shape, 0), iota(shape, 1)
    source = ((head // 2) % 2) * rings + head // 4

    def pick(first):
        wanted = source * TILE + first + head % 2
        return mm(jnp.where(line == wanted, 1.0, 0.0).astype(bf16), lines).astype(bf16)

    query = jnp.concatenate([pick(0), pick(2)], axis=1)
    turn = pick(4)[:, :ROPE]
    cached = cached_ref[...]
    score = (mm_nt(query, cached) + mm(turn, past_ref[...])) * FACTOR
    peak = jnp.max(score, axis=-1, keepdims=True)
    weight = jnp.exp(score - peak)
    total = jnp.sum(weight, axis=-1, keepdims=True)
    summed = mm(weight.astype(bf16), cached)
    sums_ref[...] = summed
    column = iota(stats_ref.shape, 1) - (stats_ref.shape[1] - ROPE // 2)
    spread = jnp.zeros(stats_ref.shape, f32)
    for k, part in enumerate((*three(peak), *three(total))):
        spread = jnp.where(column == k, part, spread)
    stats_ref[...] = spread


def chunk_kernel(lines_ref, sums_ref, stats_ref, out_ref, flat_ref):
    prompts, tiles, lanes = lines_ref.shape
    rings, lines, width = out_ref.shape
    turns = rings // 2
    flat_ref[...] = lines_ref[...].reshape(prompts * tiles, lanes).astype(f32)
    first = lax.rem(lax.axis_index("sp") // EXTRA + rings - lax.axis_index("tp_0"), turns)

    def some(k):
        return flat_ref[pl.ds(first * tiles + k, prompts // turns, stride=turns * tiles), :]

    full = [flat_ref[pl.ds(k, prompts, stride=tiles), :] for k in (0, 1, 4)]
    spare = EXTRA - prompts // turns
    stacked = jnp.concatenate(
        [
            jnp.concatenate(full[:2], axis=1),
            jnp.concatenate([some(2), some(3)], axis=1),
            jnp.zeros((spare, width // 2), f32),
        ]
    )
    count = stacked.shape[0] // 2
    latent = jnp.concatenate([stacked[:count], stacked[count:]], axis=1).astype(bf16)
    half = ROPE // 2
    turned = jnp.concatenate(
        [full[2][:, :half], some(4)[:, half:ROPE], jnp.zeros((spare, half), f32)]
    )
    turned = jnp.concatenate(
        [turned[TILE * k : TILE * (k + 1)] for k in range(2 * count // TILE)], axis=1
    )
    group = sums_ref.shape[0] // rings
    for y in range(rings):
        at = slice(group * y, group * (y + 1))
        sums = jnp.concatenate([sums_ref[at, : width // 2], sums_ref[at, width // 2 :]])
        numbers = jnp.concatenate([jnp.zeros((group, lanes), f32), stats_ref[at, :]], axis=1)
        numbers = jnp.concatenate([jnp.zeros((TILE - group, width // 2), f32), numbers])
        out_ref[y, :count, :] = latent
        out_ref[y, count:, :] = jnp.concatenate([turned + numbers, sums], axis=1).astype(bf16)


def finish_kernel(
    both_ref,
    key_ref,
    value_ref,
    nope_ref,
    turn_ref,
    place_ref,
    keys_hbm,
    values_hbm,
    rope_ref,
    out_ref,
    latent_ref,
    turned_ref,
    keys_ref,
    values_ref,
    sem,
):
    sources, lines, width = both_ref.shape
    rings = sources // 2
    count = lines - TILE
    rows = keys_ref.shape[0]
    group = 4
    half = ROPE // 2
    for y in range(rings):
        halves = []
        for c in range(2):
            source = c * rings + y
            columns = slice(c * width // 2, (c + 1) * width // 2)
            for upper in range(2):
                at = slice((2 * y + upper) * count, (2 * y + upper + 1) * count)
                latent_ref[at, columns] = both_ref[
                    source, :count, upper * width // 2 : (upper + 1) * width // 2
                ]
            packed = both_ref[source, count:, :].astype(f32)
            halves.append(
                jnp.concatenate(
                    [packed[:, half * k : half * (k + 1)] for k in range(2 * count // TILE)]
                )
            )
        at = slice(2 * y * count, 2 * (y + 1) * count)
        turned_ref[at, :] = jnp.concatenate(halves, axis=1).astype(bf16)

    third = lax.axis_index("sp") // EXTRA
    place = place_ref[0:1, :]
    for k in range(1, place_ref.shape[0]):
        place = jnp.where(third == k, place_ref[k : k + 1, :], place)
    held = latent_ref.shape[0]
    move = jnp.where(iota((rows, held), 0) == place, 1.0, 0.0).astype(bf16)
    latent = mm(move, latent_ref[...]).astype(bf16)
    turned = mm(move, turned_ref[...]).astype(bf16)
    keys = mm(latent, key_ref[...]).astype(bf16)
    keys_ref[...] = keys
    stores = [pltpu.make_async_copy(keys_ref, keys_hbm, sem.at[0])]
    stores[0].start()
    values = mm(latent, value_ref[...]).astype(bf16)
    values_ref[...] = values
    stores.append(pltpu.make_async_copy(values_ref, values_hbm, sem.at[1]))
    stores[1].start()
    same = jnp.where(iota((ROPE, ROPE), 0) == iota((ROPE, ROPE), 1), 1.0, 0.0).astype(bf16)
    rope = mm_nt(same, turned).astype(bf16)
    rope_ref[...] = rope

    nope = by_head(nope_ref[...], PLAIN_KEY_WIDTH)
    turn = by_head(turn_ref[...], ROPE)
    score = (mm_nt(nope, keys) + mm(turn, jnp.concatenate([rope, rope], axis=0))) * FACTOR

    shape = (group, 2 * ROPE)
    column = iota(shape, 1) - (2 * ROPE - half)
    mine = [(column >= k) & (column < k + 3) for k in (0, 3)]
    peaks, totals = [], []
    for source in range(sources):
        numbers = both_ref[source, count:, :].astype(f32)[group:, 2 * ROPE : 4 * ROPE]
        for found, where in zip((peaks, totals), mine):
            found.append(jnp.sum(jnp.where(where, numbers, 0.0), axis=-1, keepdims=True))
    past_peak = peaks[0]
    for x in peaks[1:]:
        past_peak = jnp.maximum(past_peak, x)
    past_total = jnp.zeros((group, 1), f32)
    past_sum = jnp.zeros((TILE, width // 2), f32)
    for k in range(sources):
        share = jnp.exp(peaks[k] - past_peak)
        past_total = past_total + totals[k] * share
        sums = both_ref[k, count:, width // 2 :].astype(f32)
        past_sum = past_sum + sums * jnp.concatenate([share, share])
    past_sum = jnp.concatenate([past_sum[:group], past_sum[group:]], axis=1)

    def own(x):
        half = group // 2
        mine = jnp.where(lax.axis_index("tp_1") == 0, x[:half], x[half:])
        return jnp.concatenate([mine, jnp.zeros((TILE - half, x.shape[1]), f32)])

    past_peak, past_total, past_sum = own(past_peak), own(past_total), own(past_sum)
    peak = jnp.maximum(past_peak, jnp.max(score, axis=-1, keepdims=True))
    share = jnp.exp(past_peak - peak)
    weight = jnp.exp(score - peak)
    denominator = past_total * share + jnp.sum(weight, axis=-1, keepdims=True)
    result = mm((past_sum * share).astype(bf16), value_ref[...]) + mm(weight.astype(bf16), values)
    result = result / denominator
    shape = result.shape
    result = jnp.where(iota(shape, 1) // VALUE_WIDTH == iota(shape, 0), result, 0.0)
    out_ref[...] = jnp.sum(result, axis=0, keepdims=True).astype(bf16)
    for store in stores:
        store.wait()


def shaped(shape, dtype=bf16):
    return jax.ShapeDtypeStruct(shape, dtype)


def limit(mib):
    return pltpu.CompilerParams(vmem_limit_bytes=mib * MIB)


def pinned(x):
    return pltpu.with_memory_space_constraint(x, pltpu.HBM)


def on_device(
    tokens,
    latent_down_weight,
    w_rope_key,
    latent_norm_gain,
    key_up_weight,
    value_up_weight,
    cached_latent_rows,
    past_rope,
    query_nope,
    query_rope,
):
    prompts, per_device, features = tokens.shape
    width = latent_down_weight.shape[1]
    row_count = prompts * per_device
    rings = lax.axis_size("tp_0")
    ring = lax.axis_index("tp_0")
    device = lax.axis_index("sp")

    places = jnp.stack([ring, rings + ring // (rings // 2)])
    positions = (PAST_POSITIONS + device * per_device + places).astype(f32)
    halfway = ROPE // 2
    frequency = rope_theta ** (-jnp.arange(halfway, dtype=f32) / halfway)
    angles = positions[:, None] * frequency

    turns = jnp.stack([jnp.cos(angles), jnp.sin(angles)])
    sources = (query_nope, query_rope, key_up_weight)
    past = (cached_latent_rows[0], past_rope[0].T)
    outgoing, turns, *past = pl.pallas_call(
        pack_kernel,
        out_shape=(
            shaped((rings, prompts + EXTRA + TILE, features)),
            shaped(turns.shape, f32),
            *(shaped(x.shape) for x in past),
        ),
        in_specs=[HBM] * 6 + [VMEM],
        out_specs=(VMEM, VMEM, ANY, ANY),
        scratch_shapes=[pltpu.VMEM(x.shape, bf16) for x in sources]
        + [pltpu.SemaphoreType.DMA((6 + rings,))],
        name="pack",
        compiler_params=limit(4),
    )(*(pinned(x) for x in (tokens.transpose(1, 0, 2), *sources, *past)), turns)
    rows = lax.all_to_all(outgoing, "tp_0", split_axis=0, concat_axis=0, tiled=True)
    rows = lax.all_gather(rows, "tp_1", axis=0, tiled=True)

    lanes = 128
    heads = 2 * lax.axis_size(TP)
    sources = (w_rope_key.T, latent_norm_gain[None], latent_down_weight)
    lines, sums, stats = pl.pallas_call(
        project_kernel,
        out_shape=(
            shaped((prompts, TILE, lanes)),
            shaped((heads, width), f32),
            shaped((heads, lanes), f32),
        ),
        in_specs=[VMEM] * 4 + [HBM] * 3,
        out_specs=(VMEM,) * 3,
        scratch_shapes=[pltpu.VMEM((prompts * TILE, lanes), f32)]
        + [pltpu.VMEM(x.shape, x.dtype) for x in sources]
        + [pltpu.SemaphoreType.DMA((rings + 2,))],
        name="project",
        compiler_params=limit(12),
    )(rows, turns, *past, *(pinned(x) for x in sources))
    arrived = lax.all_to_all(lines, "sp", split_axis=0, concat_axis=0, tiled=True)

    count = prompts + EXTRA
    chunk = pl.pallas_call(
        chunk_kernel,
        out_shape=shaped((rings, count // 2 + TILE, width)),
        in_specs=[VMEM] * 3,
        out_specs=VMEM,
        scratch_shapes=[pltpu.VMEM((prompts * TILE, lanes), f32)],
        name="chunk",
        compiler_params=limit(4),
    )(arrived, sums, stats)
    got = lax.all_to_all(chunk, "tp_0", split_axis=0, concat_axis=0, tiled=True)
    both = lax.all_gather(got, "tp_1", axis=0, tiled=True)

    turns_of = rings // 2
    y, k = np.divmod(np.arange(rings * count), count)
    tables = []
    for third in range(prompts // EXTRA):
        source = turns_of * (k - prompts) + (third - y) % turns_of
        extra = np.where(source < prompts, per_device * source + rings + y // turns_of, -1)
        tables.append(np.where(k < prompts, per_device * k + y, extra))
    keys, values, rope, attended = pl.pallas_call(
        finish_kernel,
        out_shape=(
            shaped((row_count, key_up_weight.shape[1])),
            shaped((row_count, value_up_weight.shape[1])),
            shaped((ROPE, row_count)),
            shaped((1, value_up_weight.shape[1])),
        ),
        in_specs=[VMEM] * 6,
        out_specs=(HBM, HBM, VMEM, VMEM),
        scratch_shapes=[
            pltpu.VMEM((rings * count, width), bf16),
            pltpu.VMEM((rings * count, ROPE), bf16),
            pltpu.VMEM((row_count, key_up_weight.shape[1]), bf16),
            pltpu.VMEM((row_count, value_up_weight.shape[1]), bf16),
            pltpu.SemaphoreType.DMA((2,)),
        ],
        name="finish",
        compiler_params=limit(8),
    )(
        both,
        key_up_weight,
        value_up_weight,
        query_nope,
        query_rope,
        jnp.asarray(np.stack(tables), jnp.int32),
    )
    return (keys[None], values[None], rope.T[None], attended)


def solution(mesh):
    split = Mesh(mesh.devices.reshape(mesh.shape["sp"], 8, 2), ("sp", "tp_0", "tp_1"))
    return jax.shard_map(
        on_device,
        mesh=split,
        in_specs=(
            P(None, "sp", TP),
            P(),
            P(),
            P(),
            P(None, TP),
            P(None, TP),
            P("sp", TP, None),
            P("sp", TP, None),
            P("sp", TP),
            P("sp", TP),
        ),
        out_specs=(P("sp", None, TP), P("sp", None, TP), P("sp", None, None), P("sp", TP)),
        check_vma=False,
    )
```

```python
import jax
import jax.numpy as jnp
import numpy as np
from jax import lax
from jax.experimental import pallas as pl
from jax.experimental.pallas import tpu as pltpu
from jax.sharding import Mesh
from jax.sharding import PartitionSpec as P

PLAIN_KEY_WIDTH = 128
ROPE = 64
VALUE_WIDTH = 128
PAST_POSITIONS = 32768
TP = ("tp_0", "tp_1")
EXTRA = 16
TILE = 8
FACTOR = (PLAIN_KEY_WIDTH + ROPE) ** (-0.5)

epsilon = 1e-06
rope_theta = 10000.0

VMEM = pl.BlockSpec(memory_space=pltpu.VMEM)
HBM = pl.BlockSpec(memory_space=pltpu.HBM)
MIB = 1 << 20
f32, bf16 = jnp.float32, jnp.bfloat16
NT = (((1,), (1,)), ((), ()))


def mm(a, b):
    return jnp.dot(a, b, preferred_element_type=f32)


def mm_nt(a, b):
    return lax.dot_general(a, b, NT, preferred_element_type=f32)


def iota(shape, dim):
    return lax.broadcasted_iota(jnp.int32, shape, dim)


def by_head(row, width):
    shape = (TILE, row.shape[1])
    spread = jnp.broadcast_to(row.astype(f32), shape)
    return jnp.where(iota(shape, 1) // width == iota(shape, 0), spread, 0.0).astype(bf16)


def three(x):
    high = x.astype(bf16).astype(f32)
    rest = x - high
    middle = rest.astype(bf16).astype(f32)
    return high, middle, rest - middle


def pack_kernel(
    tokens_hbm,
    nope_hbm,
    turn_hbm,
    key_hbm,
    angle_ref,
    out_ref,
    angle_out_ref,
    nope_ref,
    turn_ref,
    key_ref,
    sem,
):
    needed = [
        pltpu.make_async_copy(source, target, sem.at[k])
        for k, (source, target) in enumerate(
            ((key_hbm, key_ref), (nope_hbm, nope_ref), (turn_hbm, turn_ref))
        )
    ]
    for copy in needed:
        copy.start()
    angle_out_ref[...] = angle_ref[...]
    rings, lines, half = out_ref.shape
    prompts = tokens_hbm.shape[1]
    copies = [pltpu.make_async_copy(tokens_hbm.at[:rings], out_ref.at[:, :prompts], sem.at[3])]
    last = prompts // EXTRA - 1
    for y in range(rings):
        third = jnp.minimum(lax.rem(y % (rings // 2) + lax.axis_index("sp"), rings // 2), last)
        part = pl.ds(pl.multiple_of(third * EXTRA, EXTRA), EXTRA)
        source = tokens_hbm.at[rings + y // (rings // 2), part]
        target = out_ref.at[y, prompts : prompts + EXTRA]
        copies.append(pltpu.make_async_copy(source, target, sem.at[4 + y]))
    for copy in copies:
        copy.start()
    for copy in needed:
        copy.wait()
    latent = mm_nt(by_head(nope_ref[...], PLAIN_KEY_WIDTH), key_ref[...])
    turn = turn_ref[...].astype(f32)
    blank = jnp.zeros((1, half - ROPE), f32)
    query = [latent[0:2, :half], latent[0:2, half:]]
    query += [jnp.concatenate([turn[:, h * ROPE : (h + 1) * ROPE], blank], axis=1) for h in (0, 1)]
    query.append(jnp.zeros((2, half), f32))
    query = jnp.concatenate(query, axis=0).astype(bf16)
    for y in range(rings):
        out_ref[y, lines - TILE :, :] = query
    for copy in copies:
        copy.wait()


def project_kernel(
    rows_ref,
    angle_ref,
    turn_down_hbm,
    gain_hbm,
    down_hbm,
    out_ref,
    line_ref,
    turn_down_ref,
    gain_ref,
    down_ref,
    sem,
):
    ranks, _, features = rows_ref.shape
    rings = ranks // 2
    prompts, tiles, lanes = out_ref.shape
    count = prompts + EXTRA
    width = down_ref.shape[1]
    copies = [
        pltpu.make_async_copy(turn_down_hbm, turn_down_ref, sem.at[0]),
        pltpu.make_async_copy(gain_hbm, gain_ref, sem.at[1]),
    ]
    for y in range(rings):
        part = pl.ds(2 * y * features, 2 * features)
        copies.append(pltpu.make_async_copy(down_hbm.at[part], down_ref.at[part], sem.at[2 + y]))
    for copy in copies:
        copy.start()
    line_ref[...] = jnp.zeros_like(line_ref)
    raw = jnp.zeros((count, width), f32)
    turned = jnp.zeros((count, ROPE), f32)
    copies[0].wait()
    copies[1].wait()
    for t in range(ranks):
        x = rows_ref[(t % 2) * rings + t // 2, :count, :]
        turned = turned + mm_nt(x, turn_down_ref[:, t * features : (t + 1) * features])
    for t in range(ranks):
        if t % 2 == 0:
            copies[2 + t // 2].wait()
        x = rows_ref[(t % 2) * rings + t // 2, :count, :]
        raw = raw + mm(x, down_ref[t * features : (t + 1) * features, :])
    scale = lax.rsqrt(jnp.mean(raw * raw, axis=-1, keepdims=True) + epsilon)
    latent = raw * scale * gain_ref[...]
    first, second = turned[:, : ROPE // 2], turned[:, ROPE // 2 :]
    full = iota((count, ROPE // 2), 0) < prompts
    cos = jnp.where(full, angle_ref[0, 0:1, :], angle_ref[0, 1:2, :])
    sin = jnp.where(full, angle_ref[1, 0:1, :], angle_ref[1, 1:2, :])
    turned = jnp.where(
        lax.axis_index("tp_1") == 0, first * cos - second * sin, first * sin + second * cos
    )
    half = width // 2
    own = jnp.where(lax.axis_index("tp_1") == 0, latent[:, :half], latent[:, half:])

    def repeated(x):
        return jnp.concatenate([x[prompts:]] * (prompts // EXTRA))

    parts = [own[:prompts, :lanes], own[:prompts, lanes:]]
    parts += [repeated(own[:, :lanes]), repeated(own[:, lanes:])]
    blank = jnp.zeros((prompts, lanes - ROPE), f32)
    parts.append(jnp.concatenate([turned[:prompts], repeated(turned), blank], axis=1))
    for k, part in enumerate(parts):
        line_ref[pl.ds(k, prompts, stride=tiles), :] = part
    out_ref[...] = line_ref[...].astype(bf16).reshape(out_ref.shape)


def past_kernel(rows_ref, cached_ref, past_ref, sums_ref, stats_ref):
    ranks, count, features = rows_ref.shape
    rings = ranks // 2
    heads = 2 * ranks
    lines = rows_ref[:, count - TILE :, :].reshape(ranks * TILE, features)
    shape = (heads, ranks * TILE)
    head, line = iota(shape, 0), iota(shape, 1)
    source = ((head // 2) % 2) * rings + head // 4

    def pick(first):
        wanted = source * TILE + first + head % 2
        return mm(jnp.where(line == wanted, 1.0, 0.0).astype(bf16), lines).astype(bf16)

    query = jnp.concatenate([pick(0), pick(2)], axis=1)
    turn = pick(4)[:, :ROPE]
    cached = cached_ref[...]
    score = (mm_nt(query, cached) + mm(turn, past_ref[...])) * FACTOR
    peak = jnp.max(score, axis=-1, keepdims=True)
    weight = jnp.exp(score - peak)
    total = jnp.sum(weight, axis=-1, keepdims=True)
    summed = mm(weight.astype(bf16), cached)
    sums_ref[...] = summed
    column = iota(stats_ref.shape, 1) - (stats_ref.shape[1] - ROPE // 2)
    spread = jnp.zeros(stats_ref.shape, f32)
    for k, part in enumerate((*three(peak), *three(total))):
        spread = jnp.where(column == k, part, spread)
    stats_ref[...] = spread


def chunk_kernel(lines_ref, sums_ref, stats_ref, out_ref, flat_ref):
    prompts, tiles, lanes = lines_ref.shape
    rings, lines, width = out_ref.shape
    turns = rings // 2
    flat_ref[...] = lines_ref[...].reshape(prompts * tiles, lanes).astype(f32)
    first = lax.rem(lax.axis_index("sp") // EXTRA + rings - lax.axis_index("tp_0"), turns)

    def some(k):
        return flat_ref[pl.ds(first * tiles + k, prompts // turns, stride=turns * tiles), :]

    full = [flat_ref[pl.ds(k, prompts, stride=tiles), :] for k in (0, 1, 4)]
    spare = EXTRA - prompts // turns
    stacked = jnp.concatenate(
        [
            jnp.concatenate(full[:2], axis=1),
            jnp.concatenate([some(2), some(3)], axis=1),
            jnp.zeros((spare, width // 2), f32),
        ]
    )
    count = stacked.shape[0] // 2
    latent = jnp.concatenate([stacked[:count], stacked[count:]], axis=1).astype(bf16)
    half = ROPE // 2
    turned = jnp.concatenate(
        [full[2][:, :half], some(4)[:, half:ROPE], jnp.zeros((spare, half), f32)]
    )
    turned = jnp.concatenate(
        [turned[TILE * k : TILE * (k + 1)] for k in range(2 * count // TILE)], axis=1
    )
    group = sums_ref.shape[0] // rings
    for y in range(rings):
        at = slice(group * y, group * (y + 1))
        sums = jnp.concatenate([sums_ref[at, : width // 2], sums_ref[at, width // 2 :]])
        numbers = jnp.concatenate([jnp.zeros((group, lanes), f32), stats_ref[at, :]], axis=1)
        numbers = jnp.concatenate([jnp.zeros((TILE - group, width // 2), f32), numbers])
        out_ref[y, :count, :] = latent
        out_ref[y, count:, :] = jnp.concatenate([turned + numbers, sums], axis=1).astype(bf16)


def finish_kernel(
    both_ref,
    key_ref,
    value_ref,
    nope_ref,
    turn_ref,
    place_ref,
    keys_hbm,
    values_hbm,
    rope_ref,
    out_ref,
    latent_ref,
    turned_ref,
    keys_ref,
    values_ref,
    sem,
):
    sources, lines, width = both_ref.shape
    rings = sources // 2
    count = lines - TILE
    rows = keys_ref.shape[0]
    group = 4
    half = ROPE // 2
    for y in range(rings):
        halves = []
        for c in range(2):
            source = c * rings + y
            columns = slice(c * width // 2, (c + 1) * width // 2)
            for upper in range(2):
                at = slice((2 * y + upper) * count, (2 * y + upper + 1) * count)
                latent_ref[at, columns] = both_ref[
                    source, :count, upper * width // 2 : (upper + 1) * width // 2
                ]
            packed = both_ref[source, count:, :].astype(f32)
            halves.append(
                jnp.concatenate(
                    [packed[:, half * k : half * (k + 1)] for k in range(2 * count // TILE)]
                )
            )
        at = slice(2 * y * count, 2 * (y + 1) * count)
        turned_ref[at, :] = jnp.concatenate(halves, axis=1).astype(bf16)

    third = lax.axis_index("sp") // EXTRA
    place = place_ref[0:1, :]
    for k in range(1, place_ref.shape[0]):
        place = jnp.where(third == k, place_ref[k : k + 1, :], place)
    held = latent_ref.shape[0]
    move = jnp.where(iota((rows, held), 0) == place, 1.0, 0.0).astype(bf16)
    latent = mm(move, latent_ref[...]).astype(bf16)
    turned = mm(move, turned_ref[...]).astype(bf16)
    keys = mm(latent, key_ref[...]).astype(bf16)
    keys_ref[...] = keys
    stores = [pltpu.make_async_copy(keys_ref, keys_hbm, sem.at[0])]
    stores[0].start()
    values = mm(latent, value_ref[...]).astype(bf16)
    values_ref[...] = values
    stores.append(pltpu.make_async_copy(values_ref, values_hbm, sem.at[1]))
    stores[1].start()
    same = jnp.where(iota((ROPE, ROPE), 0) == iota((ROPE, ROPE), 1), 1.0, 0.0).astype(bf16)
    rope = mm_nt(same, turned).astype(bf16)
    rope_ref[...] = rope

    nope = by_head(nope_ref[...], PLAIN_KEY_WIDTH)
    turn = by_head(turn_ref[...], ROPE)
    score = (mm_nt(nope, keys) + mm(turn, jnp.concatenate([rope, rope], axis=0))) * FACTOR

    shape = (group, 2 * ROPE)
    column = iota(shape, 1) - (2 * ROPE - half)
    mine = [(column >= k) & (column < k + 3) for k in (0, 3)]
    peaks, totals = [], []
    for source in range(sources):
        numbers = both_ref[source, count:, :].astype(f32)[group:, 2 * ROPE : 4 * ROPE]
        for found, where in zip((peaks, totals), mine):
            found.append(jnp.sum(jnp.where(where, numbers, 0.0), axis=-1, keepdims=True))
    past_peak = peaks[0]
    for x in peaks[1:]:
        past_peak = jnp.maximum(past_peak, x)
    past_total = jnp.zeros((group, 1), f32)
    past_sum = jnp.zeros((TILE, width // 2), f32)
    for k in range(sources):
        share = jnp.exp(peaks[k] - past_peak)
        past_total = past_total + totals[k] * share
        sums = both_ref[k, count:, width // 2 :].astype(f32)
        past_sum = past_sum + sums * jnp.concatenate([share, share])
    past_sum = jnp.concatenate([past_sum[:group], past_sum[group:]], axis=1)

    def own(x):
        half = group // 2
        mine = jnp.where(lax.axis_index("tp_1") == 0, x[:half], x[half:])
        return jnp.concatenate([mine, jnp.zeros((TILE - half, x.shape[1]), f32)])

    past_peak, past_total, past_sum = own(past_peak), own(past_total), own(past_sum)
    peak = jnp.maximum(past_peak, jnp.max(score, axis=-1, keepdims=True))
    share = jnp.exp(past_peak - peak)
    weight = jnp.exp(score - peak)
    denominator = past_total * share + jnp.sum(weight, axis=-1, keepdims=True)
    result = mm((past_sum * share).astype(bf16), value_ref[...]) + mm(weight.astype(bf16), values)
    result = result / denominator
    shape = result.shape
    result = jnp.where(iota(shape, 1) // VALUE_WIDTH == iota(shape, 0), result, 0.0)
    out_ref[...] = jnp.sum(result, axis=0, keepdims=True).astype(bf16)
    for store in stores:
        store.wait()


def shaped(shape, dtype=bf16):
    return jax.ShapeDtypeStruct(shape, dtype)


def limit(mib):
    return pltpu.CompilerParams(
        vmem_limit_bytes=mib * MIB
    )


def pinned(x):
    return pltpu.with_memory_space_constraint(x, pltpu.HBM)


def on_device(
    tokens,
    latent_down_weight,
    w_rope_key,
    latent_norm_gain,
    key_up_weight,
    value_up_weight,
    cached_latent_rows,
    past_rope,
    query_nope,
    query_rope,
):
    prompts, per_device, features = tokens.shape
    width = latent_down_weight.shape[1]
    row_count = prompts * per_device
    rings = lax.axis_size("tp_0")
    ring = lax.axis_index("tp_0")
    device = lax.axis_index("sp")

    places = jnp.stack([ring, rings + ring // (rings // 2)])
    positions = (PAST_POSITIONS + device * per_device + places).astype(f32)
    halfway = ROPE // 2
    frequency = rope_theta ** (-jnp.arange(halfway, dtype=f32) / halfway)
    angles = positions[:, None] * frequency

    turns = jnp.stack([jnp.cos(angles), jnp.sin(angles)])
    sources = (query_nope, query_rope, key_up_weight)
    outgoing, turns = pl.pallas_call(
        pack_kernel,
        out_shape=(shaped((rings, prompts + EXTRA + TILE, features)), shaped(turns.shape, f32)),
        in_specs=[HBM] * 4 + [VMEM],
        out_specs=(VMEM, VMEM),
        scratch_shapes=[pltpu.VMEM(x.shape, bf16) for x in sources]
        + [pltpu.SemaphoreType.DMA((4 + rings,))],
        name="pack",
        compiler_params=limit(4),
    )(*(pinned(x) for x in (tokens.transpose(1, 0, 2), *sources)), turns)
    rows = lax.all_to_all(outgoing, "tp_0", split_axis=0, concat_axis=0, tiled=True)
    rows = lax.all_gather(rows, "tp_1", axis=0, tiled=True)

    lanes = 128
    heads = 2 * lax.axis_size(TP)
    sources = (w_rope_key.T, latent_norm_gain[None], latent_down_weight)
    lines = pl.pallas_call(
        project_kernel,
        out_shape=shaped((prompts, TILE, lanes)),
        in_specs=[VMEM] * 2 + [HBM] * 3,
        out_specs=VMEM,
        scratch_shapes=[pltpu.VMEM((prompts * TILE, lanes), f32)]
        + [pltpu.VMEM(x.shape, x.dtype) for x in sources]
        + [pltpu.SemaphoreType.DMA((rings + 2,))],
        name="project",
        compiler_params=limit(12),
    )(rows, turns, *(pinned(x) for x in sources))
    arrived = lax.all_to_all(lines, "sp", split_axis=0, concat_axis=0, tiled=True)

    sums, stats = pl.pallas_call(
        past_kernel,
        out_shape=(shaped((heads, width), f32), shaped((heads, lanes), f32)),
        in_specs=[VMEM] * 3,
        out_specs=(VMEM, VMEM),
        name="past",
        compiler_params=limit(4),
        cost_estimate=pl.CostEstimate(
            flops=300_000_000, bytes_accessed=4 * MIB, transcendentals=65536
        ),
    )(rows, cached_latent_rows[0], past_rope[0].T)

    count = prompts + EXTRA
    chunk = pl.pallas_call(
        chunk_kernel,
        out_shape=shaped((rings, count // 2 + TILE, width)),
        in_specs=[VMEM] * 3,
        out_specs=VMEM,
        scratch_shapes=[pltpu.VMEM((prompts * TILE, lanes), f32)],
        name="chunk",
        compiler_params=limit(4),
    )(arrived, sums, stats)
    got = lax.all_to_all(chunk, "tp_0", split_axis=0, concat_axis=0, tiled=True)
    both = lax.all_gather(got, "tp_1", axis=0, tiled=True)

    turns_of = rings // 2
    y, k = np.divmod(np.arange(rings * count), count)
    tables = []
    for third in range(prompts // EXTRA):
        source = turns_of * (k - prompts) + (third - y) % turns_of
        extra = np.where(source < prompts, per_device * source + rings + y // turns_of, -1)
        tables.append(np.where(k < prompts, per_device * k + y, extra))
    keys, values, rope, attended = pl.pallas_call(
        finish_kernel,
        out_shape=(
            shaped((row_count, key_up_weight.shape[1])),
            shaped((row_count, value_up_weight.shape[1])),
            shaped((ROPE, row_count)),
            shaped((1, value_up_weight.shape[1])),
        ),
        in_specs=[VMEM] * 6,
        out_specs=(HBM, HBM, VMEM, VMEM),
        scratch_shapes=[
            pltpu.VMEM((rings * count, width), bf16),
            pltpu.VMEM((rings * count, ROPE), bf16),
            pltpu.VMEM((row_count, key_up_weight.shape[1]), bf16),
            pltpu.VMEM((row_count, value_up_weight.shape[1]), bf16),
            pltpu.SemaphoreType.DMA((2,)),
        ],
        name="finish",
        compiler_params=limit(8),
    )(
        both,
        key_up_weight,
        value_up_weight,
        query_nope,
        query_rope,
        jnp.asarray(np.stack(tables), jnp.int32),
    )
    return (keys[None], values[None], rope.T[None], attended)


def solution(mesh):
    split = Mesh(mesh.devices.reshape(mesh.shape["sp"], 8, 2), ("sp", "tp_0", "tp_1"))
    return jax.shard_map(
        on_device,
        mesh=split,
        in_specs=(
            P(None, "sp", TP),
            P(),
            P(),
            P(),
            P(None, TP),
            P(None, TP),
            P("sp", TP, None),
            P("sp", TP, None),
            P("sp", TP),
            P("sp", TP),
        ),
        out_specs=(P("sp", None, TP), P("sp", None, TP), P("sp", None, None), P("sp", TP)),
        check_vma=False,
    )
```

```python
import jax
import jax.numpy as jnp
import numpy as np
from jax import lax
from jax.experimental import pallas as pl
from jax.experimental.pallas import tpu as pltpu
from jax.sharding import Mesh
from jax.sharding import PartitionSpec as P

PLAIN_KEY_WIDTH = 128
ROPE = 64
VALUE_WIDTH = 128
PAST_POSITIONS = 32768
TP = ("tp_0", "tp_1")
EXTRA = 16
TILE = 8
FACTOR = (PLAIN_KEY_WIDTH + ROPE) ** (-0.5)

epsilon = 1e-06
rope_theta = 10000.0

VMEM = pl.BlockSpec(memory_space=pltpu.VMEM)
HBM = pl.BlockSpec(memory_space=pltpu.HBM)
MIB = 1 << 20
f32, bf16 = jnp.float32, jnp.bfloat16
NT = (((1,), (1,)), ((), ()))


def mm(a, b):
    return jnp.dot(a, b, preferred_element_type=f32)


def mm_nt(a, b):
    return lax.dot_general(a, b, NT, preferred_element_type=f32)


def iota(shape, dim):
    return lax.broadcasted_iota(jnp.int32, shape, dim)


def by_head(row, width):
    shape = (TILE, row.shape[1])
    spread = jnp.broadcast_to(row.astype(f32), shape)
    return jnp.where(iota(shape, 1) // width == iota(shape, 0), spread, 0.0).astype(bf16)


def three(x):
    high = x.astype(bf16).astype(f32)
    rest = x - high
    middle = rest.astype(bf16).astype(f32)
    return high, middle, rest - middle


def pack_kernel(
    tokens_hbm,
    nope_hbm,
    turn_hbm,
    key_hbm,
    angle_ref,
    out_ref,
    angle_out_ref,
    nope_ref,
    turn_ref,
    key_ref,
    sem,
):
    needed = [
        pltpu.make_async_copy(source, target, sem.at[k])
        for k, (source, target) in enumerate(
            ((key_hbm, key_ref), (nope_hbm, nope_ref), (turn_hbm, turn_ref))
        )
    ]
    for copy in needed:
        copy.start()
    angle_out_ref[...] = angle_ref[...]
    rings, lines, half = out_ref.shape
    prompts = tokens_hbm.shape[1]
    copies = [pltpu.make_async_copy(tokens_hbm.at[:rings], out_ref.at[:, :prompts], sem.at[3])]
    last = prompts // EXTRA - 1
    for y in range(rings):
        third = jnp.minimum(lax.rem(y % (rings // 2) + lax.axis_index("sp"), rings // 2), last)
        part = pl.ds(pl.multiple_of(third * EXTRA, EXTRA), EXTRA)
        source = tokens_hbm.at[rings + y // (rings // 2), part]
        target = out_ref.at[y, prompts : prompts + EXTRA]
        copies.append(pltpu.make_async_copy(source, target, sem.at[4 + y]))
    for copy in copies:
        copy.start()
    for copy in needed:
        copy.wait()
    latent = mm_nt(by_head(nope_ref[...], PLAIN_KEY_WIDTH), key_ref[...])
    turn = turn_ref[...].astype(f32)
    blank = jnp.zeros((1, half - ROPE), f32)
    query = [latent[0:2, :half], latent[0:2, half:]]
    query += [jnp.concatenate([turn[:, h * ROPE : (h + 1) * ROPE], blank], axis=1) for h in (0, 1)]
    query.append(jnp.zeros((2, half), f32))
    query = jnp.concatenate(query, axis=0).astype(bf16)
    for y in range(rings):
        out_ref[y, lines - TILE :, :] = query
    for copy in copies:
        copy.wait()


def project_kernel(
    rows_ref,
    angle_ref,
    turn_down_hbm,
    gain_hbm,
    down_hbm,
    out_ref,
    line_ref,
    turn_down_ref,
    gain_ref,
    down_ref,
    sem,
):
    ranks, _, features = rows_ref.shape
    rings = ranks // 2
    prompts, tiles, lanes = out_ref.shape
    count = prompts + EXTRA
    width = down_ref.shape[1]
    copies = [
        pltpu.make_async_copy(turn_down_hbm, turn_down_ref, sem.at[0]),
        pltpu.make_async_copy(gain_hbm, gain_ref, sem.at[1]),
    ]
    for y in range(rings):
        part = pl.ds(2 * y * features, 2 * features)
        copies.append(pltpu.make_async_copy(down_hbm.at[part], down_ref.at[part], sem.at[2 + y]))
    for copy in copies:
        copy.start()
    line_ref[...] = jnp.zeros_like(line_ref)
    raw = jnp.zeros((count, width), f32)
    turned = jnp.zeros((count, ROPE), f32)
    copies[0].wait()
    copies[1].wait()
    for t in range(ranks):
        x = rows_ref[(t % 2) * rings + t // 2, :count, :]
        turned = turned + mm_nt(x, turn_down_ref[:, t * features : (t + 1) * features])
    for t in range(ranks):
        if t % 2 == 0:
            copies[2 + t // 2].wait()
        x = rows_ref[(t % 2) * rings + t // 2, :count, :]
        raw = raw + mm(x, down_ref[t * features : (t + 1) * features, :])
    scale = lax.rsqrt(jnp.mean(raw * raw, axis=-1, keepdims=True) + epsilon)
    latent = raw * scale * gain_ref[...]
    first, second = turned[:, : ROPE // 2], turned[:, ROPE // 2 :]
    full = iota((count, ROPE // 2), 0) < prompts
    cos = jnp.where(full, angle_ref[0, 0:1, :], angle_ref[0, 1:2, :])
    sin = jnp.where(full, angle_ref[1, 0:1, :], angle_ref[1, 1:2, :])
    turned = jnp.where(
        lax.axis_index("tp_1") == 0, first * cos - second * sin, first * sin + second * cos
    )
    half = width // 2
    own = jnp.where(lax.axis_index("tp_1") == 0, latent[:, :half], latent[:, half:])

    def repeated(x):
        return jnp.concatenate([x[prompts:]] * (prompts // EXTRA))

    parts = [own[:prompts, :lanes], own[:prompts, lanes:]]
    parts += [repeated(own[:, :lanes]), repeated(own[:, lanes:])]
    blank = jnp.zeros((prompts, lanes - ROPE), f32)
    parts.append(jnp.concatenate([turned[:prompts], repeated(turned), blank], axis=1))
    for k, part in enumerate(parts):
        line_ref[pl.ds(k, prompts, stride=tiles), :] = part
    out_ref[...] = line_ref[...].astype(bf16).reshape(out_ref.shape)


def past_kernel(
    rows_ref, cached_hbm, past_hbm, sums_ref, stats_ref, cached_ref, past_ref, sem
):
    copies = [
        pltpu.make_async_copy(cached_hbm, cached_ref, sem.at[0]),
        pltpu.make_async_copy(past_hbm, past_ref, sem.at[1]),
    ]
    for copy in copies:
        copy.start()
    ranks, count, features = rows_ref.shape
    rings = ranks // 2
    heads = 2 * ranks
    lines = rows_ref[:, count - TILE :, :].reshape(ranks * TILE, features)
    shape = (heads, ranks * TILE)
    head, line = iota(shape, 0), iota(shape, 1)
    source = ((head // 2) % 2) * rings + head // 4

    def pick(first):
        wanted = source * TILE + first + head % 2
        return mm(jnp.where(line == wanted, 1.0, 0.0).astype(bf16), lines).astype(bf16)

    query = jnp.concatenate([pick(0), pick(2)], axis=1)
    turn = pick(4)[:, :ROPE]
    for copy in copies:
        copy.wait()
    cached = cached_ref[...]
    score = (mm_nt(query, cached) + mm(turn, past_ref[...])) * FACTOR
    peak = jnp.max(score, axis=-1, keepdims=True)
    weight = jnp.exp(score - peak)
    total = jnp.sum(weight, axis=-1, keepdims=True)
    summed = mm(weight.astype(bf16), cached)
    sums_ref[...] = summed
    column = iota(stats_ref.shape, 1) - (stats_ref.shape[1] - ROPE // 2)
    spread = jnp.zeros(stats_ref.shape, f32)
    for k, part in enumerate((*three(peak), *three(total))):
        spread = jnp.where(column == k, part, spread)
    stats_ref[...] = spread


def chunk_kernel(lines_ref, sums_ref, stats_ref, out_ref, flat_ref):
    prompts, tiles, lanes = lines_ref.shape
    rings, lines, width = out_ref.shape
    turns = rings // 2
    flat_ref[...] = lines_ref[...].reshape(prompts * tiles, lanes).astype(f32)
    first = lax.rem(lax.axis_index("sp") // EXTRA + rings - lax.axis_index("tp_0"), turns)

    def some(k):
        return flat_ref[pl.ds(first * tiles + k, prompts // turns, stride=turns * tiles), :]

    full = [flat_ref[pl.ds(k, prompts, stride=tiles), :] for k in (0, 1, 4)]
    spare = EXTRA - prompts // turns
    stacked = jnp.concatenate(
        [
            jnp.concatenate(full[:2], axis=1),
            jnp.concatenate([some(2), some(3)], axis=1),
            jnp.zeros((spare, width // 2), f32),
        ]
    )
    count = stacked.shape[0] // 2
    latent = jnp.concatenate([stacked[:count], stacked[count:]], axis=1).astype(bf16)
    half = ROPE // 2
    turned = jnp.concatenate(
        [full[2][:, :half], some(4)[:, half:ROPE], jnp.zeros((spare, half), f32)]
    )
    turned = jnp.concatenate(
        [turned[TILE * k : TILE * (k + 1)] for k in range(2 * count // TILE)], axis=1
    )
    group = sums_ref.shape[0] // rings
    for y in range(rings):
        at = slice(group * y, group * (y + 1))
        sums = jnp.concatenate([sums_ref[at, : width // 2], sums_ref[at, width // 2 :]])
        numbers = jnp.concatenate([jnp.zeros((group, lanes), f32), stats_ref[at, :]], axis=1)
        numbers = jnp.concatenate([jnp.zeros((TILE - group, width // 2), f32), numbers])
        out_ref[y, :count, :] = latent
        out_ref[y, count:, :] = jnp.concatenate([turned + numbers, sums], axis=1).astype(bf16)


def finish_kernel(
    both_ref,
    key_ref,
    value_ref,
    nope_ref,
    turn_ref,
    place_ref,
    keys_hbm,
    values_hbm,
    rope_ref,
    out_ref,
    latent_ref,
    turned_ref,
    keys_ref,
    values_ref,
    sem,
):
    sources, lines, width = both_ref.shape
    rings = sources // 2
    count = lines - TILE
    rows = keys_ref.shape[0]
    group = 4
    half = ROPE // 2
    for y in range(rings):
        halves = []
        for c in range(2):
            source = c * rings + y
            columns = slice(c * width // 2, (c + 1) * width // 2)
            for upper in range(2):
                at = slice((2 * y + upper) * count, (2 * y + upper + 1) * count)
                latent_ref[at, columns] = both_ref[
                    source, :count, upper * width // 2 : (upper + 1) * width // 2
                ]
            packed = both_ref[source, count:, :].astype(f32)
            halves.append(
                jnp.concatenate(
                    [packed[:, half * k : half * (k + 1)] for k in range(2 * count // TILE)]
                )
            )
        at = slice(2 * y * count, 2 * (y + 1) * count)
        turned_ref[at, :] = jnp.concatenate(halves, axis=1).astype(bf16)

    third = lax.axis_index("sp") // EXTRA
    place = place_ref[0:1, :]
    for k in range(1, place_ref.shape[0]):
        place = jnp.where(third == k, place_ref[k : k + 1, :], place)
    held = latent_ref.shape[0]
    move = jnp.where(iota((rows, held), 0) == place, 1.0, 0.0).astype(bf16)
    latent = mm(move, latent_ref[...]).astype(bf16)
    turned = mm(move, turned_ref[...]).astype(bf16)
    keys = mm(latent, key_ref[...]).astype(bf16)
    keys_ref[...] = keys
    stores = [pltpu.make_async_copy(keys_ref, keys_hbm, sem.at[0])]
    stores[0].start()
    values = mm(latent, value_ref[...]).astype(bf16)
    values_ref[...] = values
    stores.append(pltpu.make_async_copy(values_ref, values_hbm, sem.at[1]))
    stores[1].start()
    same = jnp.where(iota((ROPE, ROPE), 0) == iota((ROPE, ROPE), 1), 1.0, 0.0).astype(bf16)
    rope = mm_nt(same, turned).astype(bf16)
    rope_ref[...] = rope

    nope = by_head(nope_ref[...], PLAIN_KEY_WIDTH)
    turn = by_head(turn_ref[...], ROPE)
    score = (mm_nt(nope, keys) + mm(turn, jnp.concatenate([rope, rope], axis=0))) * FACTOR

    shape = (group, 2 * ROPE)
    column = iota(shape, 1) - (2 * ROPE - half)
    mine = [(column >= k) & (column < k + 3) for k in (0, 3)]
    peaks, totals = [], []
    for source in range(sources):
        numbers = both_ref[source, count:, :].astype(f32)[group:, 2 * ROPE : 4 * ROPE]
        for found, where in zip((peaks, totals), mine):
            found.append(jnp.sum(jnp.where(where, numbers, 0.0), axis=-1, keepdims=True))
    past_peak = peaks[0]
    for x in peaks[1:]:
        past_peak = jnp.maximum(past_peak, x)
    past_total = jnp.zeros((group, 1), f32)
    past_sum = jnp.zeros((TILE, width // 2), f32)
    for k in range(sources):
        share = jnp.exp(peaks[k] - past_peak)
        past_total = past_total + totals[k] * share
        sums = both_ref[k, count:, width // 2 :].astype(f32)
        past_sum = past_sum + sums * jnp.concatenate([share, share])
    past_sum = jnp.concatenate([past_sum[:group], past_sum[group:]], axis=1)

    def own(x):
        half = group // 2
        mine = jnp.where(lax.axis_index("tp_1") == 0, x[:half], x[half:])
        return jnp.concatenate([mine, jnp.zeros((TILE - half, x.shape[1]), f32)])

    past_peak, past_total, past_sum = own(past_peak), own(past_total), own(past_sum)
    peak = jnp.maximum(past_peak, jnp.max(score, axis=-1, keepdims=True))
    share = jnp.exp(past_peak - peak)
    weight = jnp.exp(score - peak)
    denominator = past_total * share + jnp.sum(weight, axis=-1, keepdims=True)
    result = mm((past_sum * share).astype(bf16), value_ref[...]) + mm(weight.astype(bf16), values)
    result = result / denominator
    shape = result.shape
    result = jnp.where(iota(shape, 1) // VALUE_WIDTH == iota(shape, 0), result, 0.0)
    out_ref[...] = jnp.sum(result, axis=0, keepdims=True).astype(bf16)
    for store in stores:
        store.wait()


def shaped(shape, dtype=bf16):
    return jax.ShapeDtypeStruct(shape, dtype)


def limit(mib):
    return pltpu.CompilerParams(
        vmem_limit_bytes=mib * MIB
    )


def pinned(x):
    return pltpu.with_memory_space_constraint(x, pltpu.HBM)


def on_device(
    tokens,
    latent_down_weight,
    w_rope_key,
    latent_norm_gain,
    key_up_weight,
    value_up_weight,
    cached_latent_rows,
    past_rope,
    query_nope,
    query_rope,
):
    prompts, per_device, features = tokens.shape
    width = latent_down_weight.shape[1]
    row_count = prompts * per_device
    rings = lax.axis_size("tp_0")
    ring = lax.axis_index("tp_0")
    device = lax.axis_index("sp")

    places = jnp.stack([ring, rings + ring // (rings // 2)])
    positions = (PAST_POSITIONS + device * per_device + places).astype(f32)
    halfway = ROPE // 2
    frequency = rope_theta ** (-jnp.arange(halfway, dtype=f32) / halfway)
    angles = positions[:, None] * frequency

    turns = jnp.stack([jnp.cos(angles), jnp.sin(angles)])
    sources = (query_nope, query_rope, key_up_weight)
    outgoing, turns = pl.pallas_call(
        pack_kernel,
        out_shape=(shaped((rings, prompts + EXTRA + TILE, features)), shaped(turns.shape, f32)),
        in_specs=[HBM] * 4 + [VMEM],
        out_specs=(VMEM, VMEM),
        scratch_shapes=[pltpu.VMEM(x.shape, bf16) for x in sources]
        + [pltpu.SemaphoreType.DMA((4 + rings,))],
        name="pack",
        compiler_params=limit(4),
    )(*(pinned(x) for x in (tokens.transpose(1, 0, 2), *sources)), turns)
    rows = lax.all_to_all(outgoing, "tp_0", split_axis=0, concat_axis=0, tiled=True)
    rows = lax.all_gather(rows, "tp_1", axis=0, tiled=True)

    lanes = 128
    heads = 2 * lax.axis_size(TP)
    sources = (w_rope_key.T, latent_norm_gain[None], latent_down_weight)
    lines = pl.pallas_call(
        project_kernel,
        out_shape=shaped((prompts, TILE, lanes)),
        in_specs=[VMEM] * 2 + [HBM] * 3,
        out_specs=VMEM,
        scratch_shapes=[pltpu.VMEM((prompts * TILE, lanes), f32)]
        + [pltpu.VMEM(x.shape, x.dtype) for x in sources]
        + [pltpu.SemaphoreType.DMA((rings + 2,))],
        name="project",
        compiler_params=limit(12),
    )(rows, turns, *(pinned(x) for x in sources))
    arrived = lax.all_to_all(lines, "sp", split_axis=0, concat_axis=0, tiled=True)

    sources = (cached_latent_rows[0], past_rope[0].T)
    sums, stats = pl.pallas_call(
        past_kernel,
        out_shape=(shaped((heads, width), f32), shaped((heads, lanes), f32)),
        in_specs=[VMEM, HBM, HBM],
        out_specs=(VMEM, VMEM),
        scratch_shapes=[pltpu.VMEM(x.shape, x.dtype) for x in sources]
        + [pltpu.SemaphoreType.DMA((2,))],
        name="past",
        compiler_params=limit(8),
        cost_estimate=pl.CostEstimate(
            flops=300_000_000, bytes_accessed=4 * MIB, transcendentals=65536
        ),
    )(rows, *(pinned(x) for x in sources))

    count = prompts + EXTRA
    chunk = pl.pallas_call(
        chunk_kernel,
        out_shape=shaped((rings, count // 2 + TILE, width)),
        in_specs=[VMEM] * 3,
        out_specs=VMEM,
        scratch_shapes=[pltpu.VMEM((prompts * TILE, lanes), f32)],
        name="chunk",
        compiler_params=limit(4),
    )(arrived, sums, stats)
    got = lax.all_to_all(chunk, "tp_0", split_axis=0, concat_axis=0, tiled=True)
    both = lax.all_gather(got, "tp_1", axis=0, tiled=True)

    turns_of = rings // 2
    y, k = np.divmod(np.arange(rings * count), count)
    tables = []
    for third in range(prompts // EXTRA):
        source = turns_of * (k - prompts) + (third - y) % turns_of
        extra = np.where(source < prompts, per_device * source + rings + y // turns_of, -1)
        tables.append(np.where(k < prompts, per_device * k + y, extra))
    keys, values, rope, attended = pl.pallas_call(
        finish_kernel,
        out_shape=(
            shaped((row_count, key_up_weight.shape[1])),
            shaped((row_count, value_up_weight.shape[1])),
            shaped((ROPE, row_count)),
            shaped((1, value_up_weight.shape[1])),
        ),
        in_specs=[VMEM] * 6,
        out_specs=(HBM, HBM, VMEM, VMEM),
        scratch_shapes=[
            pltpu.VMEM((rings * count, width), bf16),
            pltpu.VMEM((rings * count, ROPE), bf16),
            pltpu.VMEM((row_count, key_up_weight.shape[1]), bf16),
            pltpu.VMEM((row_count, value_up_weight.shape[1]), bf16),
            pltpu.SemaphoreType.DMA((2,)),
        ],
        name="finish",
        compiler_params=limit(8),
    )(
        both,
        key_up_weight,
        value_up_weight,
        query_nope,
        query_rope,
        jnp.asarray(np.stack(tables), jnp.int32),
    )
    return (keys[None], values[None], rope.T[None], attended)


def solution(mesh):
    split = Mesh(mesh.devices.reshape(mesh.shape["sp"], 8, 2), ("sp", "tp_0", "tp_1"))
    return jax.shard_map(
        on_device,
        mesh=split,
        in_specs=(
            P(None, "sp", TP),
            P(),
            P(),
            P(),
            P(None, TP),
            P(None, TP),
            P("sp", TP, None),
            P("sp", TP, None),
            P("sp", TP),
            P("sp", TP),
        ),
        out_specs=(P("sp", None, TP), P("sp", None, TP), P("sp", None, None), P("sp", TP)),
        check_vma=False,
    )
```

```python
import jax
import jax.numpy as jnp
import numpy as np
from jax import lax
from jax.experimental import pallas as pl
from jax.experimental.pallas import tpu as pltpu
from jax.sharding import Mesh
from jax.sharding import PartitionSpec as P

PLAIN_KEY_WIDTH = 128
ROPE = 64
VALUE_WIDTH = 128
PAST_POSITIONS = 32768
TP = ("tp_0", "tp_1")
EXTRA = 16
TILE = 8
FACTOR = (PLAIN_KEY_WIDTH + ROPE) ** (-0.5)

epsilon = 1e-06
rope_theta = 10000.0

VMEM = pl.BlockSpec(memory_space=pltpu.VMEM)
HBM = pl.BlockSpec(memory_space=pltpu.HBM)
MIB = 1 << 20
f32, bf16 = jnp.float32, jnp.bfloat16
NT = (((1,), (1,)), ((), ()))


def mm(a, b):
    return jnp.dot(a, b, preferred_element_type=f32)


def mm_nt(a, b):
    return lax.dot_general(a, b, NT, preferred_element_type=f32)


def iota(shape, dim):
    return lax.broadcasted_iota(jnp.int32, shape, dim)


def by_head(row, width):
    shape = (TILE, row.shape[1])
    spread = jnp.broadcast_to(row.astype(f32), shape)
    return jnp.where(iota(shape, 1) // width == iota(shape, 0), spread, 0.0).astype(bf16)


def three(x):
    high = x.astype(bf16).astype(f32)
    rest = x - high
    middle = rest.astype(bf16).astype(f32)
    return high, middle, rest - middle


def pack_kernel(
    tokens_hbm,
    nope_hbm,
    turn_hbm,
    key_hbm,
    angle_ref,
    out_ref,
    angle_out_ref,
    nope_ref,
    turn_ref,
    key_ref,
    sem,
):
    needed = [
        pltpu.make_async_copy(source, target, sem.at[k])
        for k, (source, target) in enumerate(
            ((key_hbm, key_ref), (nope_hbm, nope_ref), (turn_hbm, turn_ref))
        )
    ]
    for copy in needed:
        copy.start()
    angle_out_ref[...] = angle_ref[...]
    rings, lines, half = out_ref.shape
    prompts = tokens_hbm.shape[1]
    copies = [pltpu.make_async_copy(tokens_hbm.at[:rings], out_ref.at[:, :prompts], sem.at[3])]
    last = prompts // EXTRA - 1
    for y in range(rings):
        third = jnp.minimum(lax.rem(y % (rings // 2) + lax.axis_index("sp"), rings // 2), last)
        part = pl.ds(pl.multiple_of(third * EXTRA, EXTRA), EXTRA)
        source = tokens_hbm.at[rings + y // (rings // 2), part]
        target = out_ref.at[y, prompts : prompts + EXTRA]
        copies.append(pltpu.make_async_copy(source, target, sem.at[4 + y]))
    for copy in copies:
        copy.start()
    for copy in needed:
        copy.wait()
    latent = mm_nt(by_head(nope_ref[...], PLAIN_KEY_WIDTH), key_ref[...])
    turn = turn_ref[...].astype(f32)
    blank = jnp.zeros((1, half - ROPE), f32)
    query = [latent[0:2, :half], latent[0:2, half:]]
    query += [jnp.concatenate([turn[:, h * ROPE : (h + 1) * ROPE], blank], axis=1) for h in (0, 1)]
    query.append(jnp.zeros((2, half), f32))
    query = jnp.concatenate(query, axis=0).astype(bf16)
    for y in range(rings):
        out_ref[y, lines - TILE :, :] = query
    for copy in copies:
        copy.wait()


def project_kernel(
    rows_ref,
    angle_ref,
    turn_down_hbm,
    gain_hbm,
    down_hbm,
    out_ref,
    line_ref,
    turn_down_ref,
    gain_ref,
    down_ref,
    sem,
):
    ranks, _, features = rows_ref.shape
    rings = ranks // 2
    prompts, tiles, lanes = out_ref.shape
    count = prompts + EXTRA
    width = down_ref.shape[1]
    copies = [
        pltpu.make_async_copy(turn_down_hbm, turn_down_ref, sem.at[0]),
        pltpu.make_async_copy(gain_hbm, gain_ref, sem.at[1]),
    ]
    for y in range(rings):
        part = pl.ds(2 * y * features, 2 * features)
        copies.append(pltpu.make_async_copy(down_hbm.at[part], down_ref.at[part], sem.at[2 + y]))
    for copy in copies:
        copy.start()
    line_ref[...] = jnp.zeros_like(line_ref)
    raw = jnp.zeros((count, width), f32)
    turned = jnp.zeros((count, ROPE), f32)
    copies[0].wait()
    copies[1].wait()
    for t in range(ranks):
        x = rows_ref[(t % 2) * rings + t // 2, :count, :]
        turned = turned + mm_nt(x, turn_down_ref[:, t * features : (t + 1) * features])
    for t in range(ranks):
        if t % 4 == 0:
            copies[2 + t // 2].wait()
            copies[3 + t // 2].wait()
        x = rows_ref[(t % 2) * rings + t // 2, :count, :]
        raw = raw + mm(x, down_ref[t * features : (t + 1) * features, :])
    scale = lax.rsqrt(jnp.mean(raw * raw, axis=-1, keepdims=True) + epsilon)
    latent = raw * scale * gain_ref[...]
    first, second = turned[:, : ROPE // 2], turned[:, ROPE // 2 :]
    full = iota((count, ROPE // 2), 0) < prompts
    cos = jnp.where(full, angle_ref[0, 0:1, :], angle_ref[0, 1:2, :])
    sin = jnp.where(full, angle_ref[1, 0:1, :], angle_ref[1, 1:2, :])
    turned = jnp.where(
        lax.axis_index("tp_1") == 0, first * cos - second * sin, first * sin + second * cos
    )
    half = width // 2
    own = jnp.where(lax.axis_index("tp_1") == 0, latent[:, :half], latent[:, half:])

    def repeated(x):
        return jnp.concatenate([x[prompts:]] * (prompts // EXTRA))

    parts = [own[:prompts, :lanes], own[:prompts, lanes:]]
    parts += [repeated(own[:, :lanes]), repeated(own[:, lanes:])]
    blank = jnp.zeros((prompts, lanes - ROPE), f32)
    parts.append(jnp.concatenate([turned[:prompts], repeated(turned), blank], axis=1))
    for k, part in enumerate(parts):
        line_ref[pl.ds(k, prompts, stride=tiles), :] = part
    out_ref[...] = line_ref[...].astype(bf16).reshape(out_ref.shape)


def past_kernel(
    rows_ref, cached_hbm, past_hbm, sums_ref, stats_ref, cached_ref, past_ref, sem
):
    copies = [
        pltpu.make_async_copy(cached_hbm, cached_ref, sem.at[0]),
        pltpu.make_async_copy(past_hbm, past_ref, sem.at[1]),
    ]
    for copy in copies:
        copy.start()
    ranks, count, features = rows_ref.shape
    rings = ranks // 2
    heads = 2 * ranks
    lines = rows_ref[:, count - TILE :, :].reshape(ranks * TILE, features)
    shape = (heads, ranks * TILE)
    head, line = iota(shape, 0), iota(shape, 1)
    source = ((head // 2) % 2) * rings + head // 4

    def pick(first):
        wanted = source * TILE + first + head % 2
        return mm(jnp.where(line == wanted, 1.0, 0.0).astype(bf16), lines).astype(bf16)

    query = jnp.concatenate([pick(0), pick(2)], axis=1)
    turn = pick(4)[:, :ROPE]
    for copy in copies:
        copy.wait()
    cached = cached_ref[...]
    score = (mm_nt(query, cached) + mm(turn, past_ref[...])) * FACTOR
    peak = jnp.max(score, axis=-1, keepdims=True)
    weight = jnp.exp(score - peak)
    total = jnp.sum(weight, axis=-1, keepdims=True)
    summed = mm(weight.astype(bf16), cached)
    sums_ref[...] = summed
    column = iota(stats_ref.shape, 1) - (stats_ref.shape[1] - ROPE // 2)
    spread = jnp.zeros(stats_ref.shape, f32)
    for k, part in enumerate((*three(peak), *three(total))):
        spread = jnp.where(column == k, part, spread)
    stats_ref[...] = spread


def chunk_kernel(lines_ref, sums_ref, stats_ref, out_ref, flat_ref):
    prompts, tiles, lanes = lines_ref.shape
    rings, lines, width = out_ref.shape
    turns = rings // 2
    flat_ref[...] = lines_ref[...].reshape(prompts * tiles, lanes).astype(f32)
    first = lax.rem(lax.axis_index("sp") // EXTRA + rings - lax.axis_index("tp_0"), turns)

    def some(k):
        return flat_ref[pl.ds(first * tiles + k, prompts // turns, stride=turns * tiles), :]

    full = [flat_ref[pl.ds(k, prompts, stride=tiles), :] for k in (0, 1, 4)]
    spare = EXTRA - prompts // turns
    stacked = jnp.concatenate(
        [
            jnp.concatenate(full[:2], axis=1),
            jnp.concatenate([some(2), some(3)], axis=1),
            jnp.zeros((spare, width // 2), f32),
        ]
    )
    count = stacked.shape[0] // 2
    latent = jnp.concatenate([stacked[:count], stacked[count:]], axis=1).astype(bf16)
    half = ROPE // 2
    turned = jnp.concatenate(
        [full[2][:, :half], some(4)[:, half:ROPE], jnp.zeros((spare, half), f32)]
    )
    turned = jnp.concatenate(
        [turned[TILE * k : TILE * (k + 1)] for k in range(2 * count // TILE)], axis=1
    )
    group = sums_ref.shape[0] // rings
    for y in range(rings):
        at = slice(group * y, group * (y + 1))
        sums = jnp.concatenate([sums_ref[at, : width // 2], sums_ref[at, width // 2 :]])
        numbers = jnp.concatenate([jnp.zeros((group, lanes), f32), stats_ref[at, :]], axis=1)
        numbers = jnp.concatenate([jnp.zeros((TILE - group, width // 2), f32), numbers])
        out_ref[y, :count, :] = latent
        out_ref[y, count:, :] = jnp.concatenate([turned + numbers, sums], axis=1).astype(bf16)


def finish_kernel(
    both_ref,
    key_ref,
    value_ref,
    nope_ref,
    turn_ref,
    place_ref,
    keys_hbm,
    values_hbm,
    rope_ref,
    out_ref,
    latent_ref,
    turned_ref,
    keys_ref,
    values_ref,
    sem,
):
    sources, lines, width = both_ref.shape
    rings = sources // 2
    count = lines - TILE
    rows = keys_ref.shape[0]
    group = 4
    half = ROPE // 2
    for y in range(rings):
        halves = []
        for c in range(2):
            source = c * rings + y
            columns = slice(c * width // 2, (c + 1) * width // 2)
            for upper in range(2):
                at = slice((2 * y + upper) * count, (2 * y + upper + 1) * count)
                latent_ref[at, columns] = both_ref[
                    source, :count, upper * width // 2 : (upper + 1) * width // 2
                ]
            packed = both_ref[source, count:, :].astype(f32)
            halves.append(
                jnp.concatenate(
                    [packed[:, half * k : half * (k + 1)] for k in range(2 * count // TILE)]
                )
            )
        at = slice(2 * y * count, 2 * (y + 1) * count)
        turned_ref[at, :] = jnp.concatenate(halves, axis=1).astype(bf16)

    third = lax.axis_index("sp") // EXTRA
    place = place_ref[0:1, :]
    for k in range(1, place_ref.shape[0]):
        place = jnp.where(third == k, place_ref[k : k + 1, :], place)
    held = latent_ref.shape[0]
    move = jnp.where(iota((rows, held), 0) == place, 1.0, 0.0).astype(bf16)
    latent = mm(move, latent_ref[...]).astype(bf16)
    turned = mm(move, turned_ref[...]).astype(bf16)
    keys = mm(latent, key_ref[...]).astype(bf16)
    keys_ref[...] = keys
    values = mm(latent, value_ref[...]).astype(bf16)
    values_ref[...] = values
    same = jnp.where(iota((ROPE, ROPE), 0) == iota((ROPE, ROPE), 1), 1.0, 0.0).astype(bf16)
    rope = mm_nt(same, turned).astype(bf16)
    rope_ref[...] = rope

    nope = by_head(nope_ref[...], PLAIN_KEY_WIDTH)
    turn = by_head(turn_ref[...], ROPE)
    score = (mm_nt(nope, keys) + mm(turn, jnp.concatenate([rope, rope], axis=0))) * FACTOR

    shape = (group, 2 * ROPE)
    column = iota(shape, 1) - (2 * ROPE - half)
    mine = [(column >= k) & (column < k + 3) for k in (0, 3)]
    peaks, totals = [], []
    for source in range(sources):
        numbers = both_ref[source, count:, :].astype(f32)[group:, 2 * ROPE : 4 * ROPE]
        for found, where in zip((peaks, totals), mine):
            found.append(jnp.sum(jnp.where(where, numbers, 0.0), axis=-1, keepdims=True))
    past_peak = peaks[0]
    for x in peaks[1:]:
        past_peak = jnp.maximum(past_peak, x)
    past_total = jnp.zeros((group, 1), f32)
    past_sum = jnp.zeros((TILE, width // 2), f32)
    for k in range(sources):
        share = jnp.exp(peaks[k] - past_peak)
        past_total = past_total + totals[k] * share
        sums = both_ref[k, count:, width // 2 :].astype(f32)
        past_sum = past_sum + sums * jnp.concatenate([share, share])
    past_sum = jnp.concatenate([past_sum[:group], past_sum[group:]], axis=1)

    def own(x):
        half = group // 2
        mine = jnp.where(lax.axis_index("tp_1") == 0, x[:half], x[half:])
        return jnp.concatenate([mine, jnp.zeros((TILE - half, x.shape[1]), f32)])

    stores = [
        pltpu.make_async_copy(keys_ref, keys_hbm, sem.at[0]),
        pltpu.make_async_copy(values_ref, values_hbm, sem.at[1]),
    ]
    for store in stores:
        store.start()
    past_peak, past_total, past_sum = own(past_peak), own(past_total), own(past_sum)
    peak = jnp.maximum(past_peak, jnp.max(score, axis=-1, keepdims=True))
    share = jnp.exp(past_peak - peak)
    weight = jnp.exp(score - peak)
    denominator = past_total * share + jnp.sum(weight, axis=-1, keepdims=True)
    result = mm((past_sum * share).astype(bf16), value_ref[...]) + mm(weight.astype(bf16), values)
    result = result / denominator
    shape = result.shape
    result = jnp.where(iota(shape, 1) // VALUE_WIDTH == iota(shape, 0), result, 0.0)
    out_ref[...] = jnp.sum(result, axis=0, keepdims=True).astype(bf16)
    for store in stores:
        store.wait()


def shaped(shape, dtype=bf16):
    return jax.ShapeDtypeStruct(shape, dtype)


def limit(mib):
    return pltpu.CompilerParams(
        vmem_limit_bytes=mib * MIB
    )


def pinned(x):
    return pltpu.with_memory_space_constraint(x, pltpu.HBM)


def on_device(
    tokens,
    latent_down_weight,
    w_rope_key,
    latent_norm_gain,
    key_up_weight,
    value_up_weight,
    cached_latent_rows,
    past_rope,
    query_nope,
    query_rope,
):
    prompts, per_device, features = tokens.shape
    width = latent_down_weight.shape[1]
    row_count = prompts * per_device
    rings = lax.axis_size("tp_0")
    ring = lax.axis_index("tp_0")
    device = lax.axis_index("sp")

    places = jnp.stack([ring, rings + ring // (rings // 2)])
    positions = (PAST_POSITIONS + device * per_device + places).astype(f32)
    halfway = ROPE // 2
    frequency = rope_theta ** (-jnp.arange(halfway, dtype=f32) / halfway)
    angles = positions[:, None] * frequency

    turns = jnp.stack([jnp.cos(angles), jnp.sin(angles)])
    sources = (query_nope, query_rope, key_up_weight)
    outgoing, turns = pl.pallas_call(
        pack_kernel,
        out_shape=(shaped((rings, prompts + EXTRA + TILE, features)), shaped(turns.shape, f32)),
        in_specs=[HBM] * 4 + [VMEM],
        out_specs=(VMEM, VMEM),
        scratch_shapes=[pltpu.VMEM(x.shape, bf16) for x in sources]
        + [pltpu.SemaphoreType.DMA((4 + rings,))],
        name="pack",
        compiler_params=limit(4),
    )(*(pinned(x) for x in (tokens.transpose(1, 0, 2), *sources)), turns)
    rows = lax.all_to_all(outgoing, "tp_0", split_axis=0, concat_axis=0, tiled=True)
    rows = lax.all_gather(rows, "tp_1", axis=0, tiled=True)

    lanes = 128
    heads = 2 * lax.axis_size(TP)
    sources = (w_rope_key.T, latent_norm_gain[None], latent_down_weight)
    lines = pl.pallas_call(
        project_kernel,
        out_shape=shaped((prompts, TILE, lanes)),
        in_specs=[VMEM] * 2 + [HBM] * 3,
        out_specs=VMEM,
        scratch_shapes=[pltpu.VMEM((prompts * TILE, lanes), f32)]
        + [pltpu.VMEM(x.shape, x.dtype) for x in sources]
        + [pltpu.SemaphoreType.DMA((rings + 2,))],
        name="project",
        compiler_params=limit(12),
    )(rows, turns, *(pinned(x) for x in sources))
    arrived = lax.all_to_all(lines, "sp", split_axis=0, concat_axis=0, tiled=True)

    sources = (cached_latent_rows[0], past_rope[0].T)
    sums, stats = pl.pallas_call(
        past_kernel,
        out_shape=(shaped((heads, width), f32), shaped((heads, lanes), f32)),
        in_specs=[VMEM, HBM, HBM],
        out_specs=(VMEM, VMEM),
        scratch_shapes=[pltpu.VMEM(x.shape, x.dtype) for x in sources]
        + [pltpu.SemaphoreType.DMA((2,))],
        name="past",
        compiler_params=limit(8),
        cost_estimate=pl.CostEstimate(
            flops=300_000_000, bytes_accessed=4 * MIB, transcendentals=65536
        ),
    )(rows, *(pinned(x) for x in sources))

    count = prompts + EXTRA
    chunk = pl.pallas_call(
        chunk_kernel,
        out_shape=shaped((rings, count // 2 + TILE, width)),
        in_specs=[VMEM] * 3,
        out_specs=VMEM,
        scratch_shapes=[pltpu.VMEM((prompts * TILE, lanes), f32)],
        name="chunk",
        compiler_params=limit(4),
    )(arrived, sums, stats)
    got = lax.all_to_all(chunk, "tp_0", split_axis=0, concat_axis=0, tiled=True)
    both = lax.all_gather(got, "tp_1", axis=0, tiled=True)

    turns_of = rings // 2
    y, k = np.divmod(np.arange(rings * count), count)
    tables = []
    for third in range(prompts // EXTRA):
        source = turns_of * (k - prompts) + (third - y) % turns_of
        extra = np.where(source < prompts, per_device * source + rings + y // turns_of, -1)
        tables.append(np.where(k < prompts, per_device * k + y, extra))
    keys, values, rope, attended = pl.pallas_call(
        finish_kernel,
        out_shape=(
            shaped((row_count, key_up_weight.shape[1])),
            shaped((row_count, value_up_weight.shape[1])),
            shaped((ROPE, row_count)),
            shaped((1, value_up_weight.shape[1])),
        ),
        in_specs=[VMEM] * 6,
        out_specs=(HBM, HBM, VMEM, VMEM),
        scratch_shapes=[
            pltpu.VMEM((rings * count, width), bf16),
            pltpu.VMEM((rings * count, ROPE), bf16),
            pltpu.VMEM((row_count, key_up_weight.shape[1]), bf16),
            pltpu.VMEM((row_count, value_up_weight.shape[1]), bf16),
            pltpu.SemaphoreType.DMA((2,)),
        ],
        name="finish",
        compiler_params=limit(8),
    )(
        both,
        key_up_weight,
        value_up_weight,
        query_nope,
        query_rope,
        jnp.asarray(np.stack(tables), jnp.int32),
    )
    return (keys[None], values[None], rope.T[None], attended)


def solution(mesh):
    split = Mesh(mesh.devices.reshape(mesh.shape["sp"], 8, 2), ("sp", "tp_0", "tp_1"))
    return jax.shard_map(
        on_device,
        mesh=split,
        in_specs=(
            P(None, "sp", TP),
            P(),
            P(),
            P(),
            P(None, TP),
            P(None, TP),
            P("sp", TP, None),
            P("sp", TP, None),
            P("sp", TP),
            P("sp", TP),
        ),
        out_specs=(P("sp", None, TP), P("sp", None, TP), P("sp", None, None), P("sp", TP)),
        check_vma=False,
    )
```
